256 devices in a mesh: ep: 64 (over z, y, core), tp: 4 (over x).
Axes of the slice: x: 4, y: 4, z: 8, core: 2. Of those that a mesh axis runs over, the one named last changes fastest.
Arguments:
- mixer_in: bfloat16 [24576, 2048], P(('ep', 'tp')), may hold values from -6 to 6
- expert_in: bfloat16 [24576, 2048], P(('ep', 'tp')), may hold values from -6 to 6
- mixer_gain: float32 [2048], replicated, may hold values from 0.1 to 1.9
- in_gate_weight: bfloat16 [2048, 2048], P(None, 'tp'), may hold values from -0.125 to 0.125
- out_gate_weight: bfloat16 [2048, 2048], P(None, 'tp'), may hold values from -0.125 to 0.125
- value_weight: bfloat16 [2048, 2048], P(None, 'tp'), may hold values from -0.125 to 0.125
- conv_taps: float32 [3, 2048], replicated, may hold values from -3 to 3
- mixer_proj: bfloat16 [2048, 2048], P(None, 'tp'), may hold values from -0.125 to 0.125
- expert_gain: float32 [2048], replicated, may hold values from 0.1 to 1.9
- route_ids: int32 [24576, 2], P('ep'), may hold values from 0 to 63, all different within a row; in each aligned block of 96 rows (0 to 95, 96 to 191, ...) at most 6 rows name the same one
- route_weights: float32 [24576, 2], P('ep'), may hold values from 0.1 to 1
- gate_weight: bfloat16 [64, 2048, 1024], P('ep', None, 'tp'), may hold values from -0.125 to 0.125
- up_weight: bfloat16 [64, 2048, 1024], P('ep', None, 'tp'), may hold values from -0.125 to 0.125
- down_weight: bfloat16 [64, 1024, 2048], P('ep', None, 'tp'), may hold values from -0.1875 to 0.1875
Outputs:
- mixer_out: bfloat16 [24576, 2048], P('ep', 'tp')
- expert_out: bfloat16 [24576, 2048], P('ep', 'tp')
The draws below stay inside these ranges and needn't reach their ends.
Inputs may be any that keep to these rules, and one draw needn't show every extreme that they name: `route_ids`: each row names 2 different experts. In each aligned block of 96 rows no expert is named by more than 6 rows, a bound that some block reaches.
All inputs are finite; a program needn't handle non-finite values.
Results may differ from the reference program's by a relative error of at most 0.0076.
Values may be sent and summed in bfloat16 or wider, within the bound.
A program may use at most 64 MiB of HBM per device.

```python
import math
import jax
import jax.numpy as jnp
import numpy as np
from jax import lax

D = 2048
F = 1024
CONV = 3
TOP_K = 2
TOK_DEV = 96
EXPERTS = 64
CAPQ = 6
TOKENS = 24576
N_EP = 64
N_TP = 4


def shard_levels(rng, extent, pieces, low, high):
    def one(position, blocks):
        draws = jax.random.uniform(jax.random.fold_in(jax.random.fold_in(rng, 6), position), (blocks,), jnp.float32, low / len(pieces), high / len(pieces))
        return jnp.repeat(jnp.exp(draws), extent[position] // blocks).reshape((-1,) + (1,) * (len(extent) - position - 1))

    level = one(*pieces[0])
    for cut in pieces[1:]:
        level = level * one(*cut)
    return level


def routed_block(own_key, own, number, rows, amount, top, limit, slope):
    order = jax.random.permutation(own_key, amount)
    heavy_load, common = portions_of(amount, rows * top, limit, slope, True), portions_of(amount, rows * top, limit, slope, False)
    places = jnp.arange(amount)

    def named(lengths, rotation):
        used = int((lengths > 0).sum())
        fixed = max(1, used // 4)
        passed = fixed + (places - fixed + rotation * (used - fixed)) % max(1, amount - fixed)
        return jnp.zeros((amount,), jnp.int32).at[order[jnp.where(places < fixed, places, passed)]].set(jnp.asarray(lengths, jnp.int32))

    lengths = jnp.where(number % 4 == 0, named(heavy_load, number // 4), named(common, number - number // 4 - 1))
    mixed = jax.random.permutation(jax.random.fold_in(own, 3), amount)
    donor, receiver = mixed[0:amount // 2 * 2:2], mixed[1:amount // 2 * 2:2]
    margin = jnp.minimum(lengths[donor] - 1, limit - lengths[receiver]) // 2
    margin = jnp.where((donor == order[0]) | (receiver == order[0]) | (lengths[receiver] == 0), 0, jnp.maximum(margin, 0))
    passed = jax.random.randint(jax.random.fold_in(own, 4), (amount // 2,), 0, 1 << 20) % (margin + 1)
    lengths = lengths.at[donor].add(-passed).at[receiver].add(passed)
    items = jnp.searchsorted(jnp.cumsum(lengths), jnp.arange(rows * top), side="right").astype(jnp.int32)
    table = items.reshape(top, rows).T
    table = table[jax.random.permutation(jax.random.fold_in(own, 1), rows)]
    rotation = jax.random.randint(jax.random.fold_in(own, 2), (rows, 1), 0, top)
    return jnp.take_along_axis(table, (jnp.arange(top)[None, :] + rotation) % top, axis=1)


def portions_of(count, total, most, skew, full):
    loads = [(1 << 20) // math.isqrt(standing ** skew) + 1 for standing in range(1, count + 1)]
    largest = most if full else min(most, max(-(-total // count), total * loads[0] // sum(loads)))
    least = 1 if total - largest >= count - 1 else 0
    given, surplus = [largest] + [least] * (count - 1), total - largest - least * (count - 1)
    while surplus > 0:
        candidates = [i for i in range(1, count) if given[i] < largest] or [i for i in range(1, count) if given[i] < most]
        mass, left = sum([loads[i] for i in candidates]), surplus
        for i in candidates:
            extra = min(most - given[i], max(1, left * loads[i] // mass), surplus)
            given[i] = given[i] + extra
            surplus = surplus - extra
    return np.array(given)


def centred(stream_key, dims, width, limit, pieces=(), held_as=jnp.bfloat16):
    loudness = shard_levels(stream_key, dims, pieces, -0.22, 0.18) if pieces else 1.0
    entries = jax.random.normal(stream_key, dims, jnp.float32) * width * loudness
    return jnp.minimum(jnp.maximum(entries, -limit), limit).astype(held_as)


def setup_inputs(seed: int = 0) -> dict:
    key_of = jax.random.split(jax.random.key(seed), 15)
    mixer_in = centred(key_of[0], (TOKENS, D), 1.0, 6.0, ((0, 256),))
    expert_in = centred(key_of[1], (TOKENS, D), 1.0, 6.0, ((0, 256),))
    mixer_gain = jnp.clip(1.0 + 0.18 * jax.random.normal(key_of[2], (D,), jnp.float32), 0.1, 1.9)
    in_gate_weight = centred(key_of[3], (D, D), D ** -0.5, 0.125, ((1, 4),))
    out_gate_weight = centred(key_of[4], (D, D), D ** -0.5, 0.125, ((1, 4),))
    value_weight = centred(key_of[5], (D, D), D ** -0.5, 0.125, ((1, 4),))
    conv_taps = centred(key_of[6], (CONV, D), 0.577, 3.0, (), jnp.float32)
    mixer_proj = centred(key_of[7], (D, D), D ** -0.5, 0.125, ((1, 4),))
    expert_gain = jnp.clip(1.0 + 0.18 * jax.random.normal(key_of[8], (D,), jnp.float32), 0.1, 1.9)
    route_ids_keys = jax.random.split(jax.random.fold_in(key_of[9], 1), TOKENS // TOK_DEV)
    route_ids_turns = jax.random.permutation(jax.random.fold_in(key_of[9], 3), TOKENS // TOK_DEV)
    route_ids = jax.vmap(lambda own, number: routed_block(jax.random.fold_in(key_of[9], 2), own, number, TOK_DEV, EXPERTS, TOP_K, CAPQ, 1))(route_ids_keys, route_ids_turns).reshape((TOKENS, TOP_K))
    route_weights = jnp.clip(jnp.exp(math.log(1.0) - 2.3025851 * jax.random.uniform(key_of[10], (TOKENS, TOP_K), jnp.float32) ** shard_levels(key_of[10], (TOKENS, TOP_K), ((0, 64),), -0.2, 0.2)), 0.1, 1.0)
    gate_weight = centred(key_of[11], (EXPERTS, D, F), D ** -0.5, 0.125, ((0, 64), (2, 4)))
    up_weight = centred(key_of[12], (EXPERTS, D, F), D ** -0.5, 0.125, ((0, 64), (2, 4)))
    down_weight = centred(key_of[13], (EXPERTS, F, D), F ** -0.5, 0.1875, ((0, 64), (2, 4)))
    return dict(mixer_in=mixer_in, expert_in=expert_in, mixer_gain=mixer_gain, in_gate_weight=in_gate_weight, out_gate_weight=out_gate_weight, value_weight=value_weight, conv_taps=conv_taps, mixer_proj=mixer_proj, expert_gain=expert_gain, route_ids=route_ids, route_weights=route_weights, gate_weight=gate_weight, up_weight=up_weight, down_weight=down_weight)


norm_eps = 1e-06

def rms_rows(values, gain_row):
    wide = values.astype(jnp.float32)
    scale = lax.rsqrt(lax.optimization_barrier(jnp.mean(wide * wide, axis=-1, keepdims=True)) + norm_eps)
    return (wide * scale * gain_row.astype(jnp.float32)).astype(jnp.bfloat16)

def place_slots(route_ids, group_rows, experts, slot_cap):
    row_total, top_count = route_ids.shape
    groups = row_total // group_rows
    labels = jnp.arange(experts, dtype=jnp.int32)
    onehot = (route_ids.reshape(groups, group_rows * top_count)[:, :, None] == labels[None, None, :]).astype(jnp.int32)
    earlier = jnp.cumsum(onehot, axis=1) - onehot
    within = lax.optimization_barrier(jnp.sum(earlier * onehot, axis=2))
    slot_index = jnp.arange(groups, dtype=jnp.int32)[:, None] * slot_cap + within
    return slot_index.reshape(row_total, top_count).astype(jnp.int32)

def reference(mixer_in, expert_in, mixer_gain, in_gate_weight, out_gate_weight, value_weight, conv_taps, mixer_proj, expert_gain, route_ids, route_weights, gate_weight, up_weight, down_weight):
    mixer_normed = rms_rows(mixer_in, mixer_gain)
    in_gate = jnp.dot(mixer_normed, in_gate_weight, preferred_element_type=jnp.float32)
    out_gate = jnp.dot(mixer_normed, out_gate_weight, preferred_element_type=jnp.float32)
    values = jnp.dot(mixer_normed, value_weight, preferred_element_type=jnp.float32)
    product = (in_gate * values).astype(jnp.bfloat16)
    product = lax.optimization_barrier(product)
    row_count = product.shape[0]
    tap_count = conv_taps.shape[0]
    padded = jnp.pad(product.astype(jnp.float32), ((tap_count - 1, 0), (0, 0)))
    tap_rows = conv_taps.astype(jnp.float32)
    conv_sum = tap_rows[0] * padded[0:row_count]
    for tap_index in range(1, tap_count):
        conv_sum = conv_sum + tap_rows[tap_index] * padded[tap_index:tap_index + row_count]
    gated = (out_gate * conv_sum).astype(jnp.bfloat16)
    mixer_out = jnp.dot(gated, mixer_proj, preferred_element_type=jnp.float32).astype(jnp.bfloat16)
    expert_normed = rms_rows(expert_in, expert_gain)
    token_count = expert_normed.shape[0]
    top_count = route_ids.shape[1]
    per_expert = N_EP * N_TP * CAPQ
    slot_index = place_slots(route_ids, TOK_DEV, EXPERTS, CAPQ)
    flat_index = (route_ids * per_expert + slot_index).reshape(-1)
    shares = (route_weights / lax.optimization_barrier(jnp.sum(route_weights, axis=1, keepdims=True))).reshape(-1)
    row_table = jnp.full((EXPERTS * per_expert,), token_count, jnp.int32).at[flat_index].set(jnp.repeat(jnp.arange(token_count, dtype=jnp.int32), top_count))
    share_table = jnp.zeros((EXPERTS * per_expert,), jnp.float32).at[flat_index].set(shares)
    padded_rows = jnp.concatenate([expert_normed, jnp.zeros((1, expert_normed.shape[1]), jnp.bfloat16)], axis=0)

    def one_expert(running, expert_idx):
        rows_here = lax.dynamic_slice_in_dim(row_table, expert_idx * per_expert, per_expert)
        share_here = lax.dynamic_slice_in_dim(share_table, expert_idx * per_expert, per_expert)
        chosen = padded_rows[rows_here]
        gate_pre = jnp.dot(chosen, gate_weight[expert_idx], preferred_element_type=jnp.float32)
        up_pre = jnp.dot(chosen, up_weight[expert_idx], preferred_element_type=jnp.float32)
        hidden = (jax.nn.silu(gate_pre) * up_pre).astype(jnp.bfloat16)
        result = jnp.dot(hidden, down_weight[expert_idx], preferred_element_type=jnp.float32).astype(jnp.bfloat16)
        running = running.at[rows_here].add(share_here[:, None] * result.astype(jnp.float32))
        return (running, None)
    running, _ = lax.scan(one_expert, jnp.zeros((token_count + 1, expert_normed.shape[1]), jnp.float32), jnp.arange(EXPERTS, dtype=jnp.int32))
    expert_out = running[:token_count].astype(jnp.bfloat16)
    return (mixer_out, expert_out)
```

```python
import jax
import jax.numpy as jnp
from jax import lax
from jax.experimental import pallas as pl
from jax.experimental.pallas import tpu as pltpu
from jax.sharding import PartitionSpec as P

norm_eps = 1e-06
Z, Y, C, X = 8, 4, 2, 4
PLANE = Y * C
EP = Z * PLANE
CAP = 24
MESH = pl.DeviceIdType.MESH


def rms_rows(values, gain_row):
    wide = values.astype(jnp.float32)
    scale = lax.rsqrt(jnp.mean(wide * wide, axis=-1, keepdims=True) + norm_eps)
    return (wide * scale * gain_row).astype(jnp.bfloat16)


def offset_of(step):
    forth, back = 1 + step // 2, Z - (step + 1) // 2
    dz = jnp.where(lax.rem(step, 2) == 0, forth, back)
    return jnp.where(step == Z - 1, 0, dz)


def kernel(
    mixer_in, expert_in, mixer_gain, expert_gain, taps, ids, weights,
    wi_hbm, wo_hbm, wv_hbm, wp_hbm, wg_hbm, wu_hbm, wd_hbm,
    mixer_out, expert_out,
    wi, wo, wv, wp, wg, wu, wd,
    tok_send, tok, mrows, send, rows, hid, res, ret, gat, ext, ogate, acc, rim_s, rim_r, slot_rows, cols,
    load_sem, tok_ss, tok_rs, mix_ss, mix_rs, disp_ss, disp_rs, row_ss, row_rs, hid_ss, hid_rs,
    ret_ss, ret_rs, gat_ss, gat_rs, rim_ss, rim_rs,
):
    ep, tp = lax.axis_index("ep"), lax.axis_index("tp")
    z = ep // PLANE
    right, left, far = lax.rem(tp + 1, X), lax.rem(tp + 3, X), lax.rem(tp + 2, X)

    loads = [
        pltpu.make_async_copy(src, dst, load_sem.at[i])
        for i, (src, dst) in enumerate(
            ((wi_hbm, wi), (wo_hbm, wo), (wv_hbm, wv), (wg_hbm, wg), (wu_hbm, wu), (wd_hbm, wd), (wp_hbm, wp))
        )
    ]
    for load in loads:
        load.start()

    barrier = pltpu.get_barrier_semaphore()

    @pl.loop(1, EP)
    def _(d):
        pl.semaphore_signal(barrier, inc=1, device_id={"ep": lax.rem(ep + d, EP)}, device_id_type=MESH)

    for other in (right, left, far):
        pl.semaphore_signal(barrier, inc=1, device_id={"tp": other}, device_id_type=MESH)

    def to_ep(src, dst, ss, rs, target):
        return pltpu.make_async_remote_copy(src, dst, ss, rs, device_id={"ep": target}, device_id_type=MESH)

    def to_tp(src, dst, ss, rs, target):
        return pltpu.make_async_remote_copy(src, dst, ss, rs, device_id={"tp": target}, device_id_type=MESH)

    def await_recv(ref, sem):
        to_tp(ref, ref, sem, sem, right).wait_recv()

    def await_send(ref, sem):
        to_tp(ref, ref, sem, sem, right).wait_send()

    normed = rms_rows(expert_in[...], expert_gain[...])
    for k in range(X):
        tok_send[k] = normed[:, k * 512 : (k + 1) * 512]
    mrows[tp] = rms_rows(mixer_in[...], mixer_gain[...])
    tok[tp] = tok_send[tp]

    pl.semaphore_wait(barrier, EP + 2)

    for i, other in enumerate((right, left, far)):
        to_tp(tok_send.at[other], tok.at[tp], tok_ss, tok_rs, other).start()
    to_tp(mrows.at[tp], mrows.at[tp], mix_ss.at[0], mix_rs.at[0], right).start()
    to_tp(mrows.at[tp], mrows.at[tp], mix_ss.at[1], mix_rs.at[1], left).start()

    count = ids.shape[1]
    labels = lax.broadcasted_iota(jnp.int32, (EP, count), 0)
    hot = [ids[k : k + 1, :] == labels for k in range(2)]
    named = jnp.where(hot[0] | hot[1], 1.0, 0.0).astype(jnp.bfloat16)
    older = (
        lax.broadcasted_iota(jnp.int32, (count, count), 0) < lax.broadcasted_iota(jnp.int32, (count, count), 1)
    )
    earlier = jnp.dot(named, jnp.where(older, 1.0, 0.0).astype(jnp.bfloat16), preferred_element_type=jnp.float32)
    total = weights[0:1, :] + weights[1:2, :]
    for k in range(2):
        within = jnp.sum(jnp.where(hot[k], earlier, 0.0), axis=0, keepdims=True)
        slot = ids[k : k + 1, :].astype(jnp.float32) * CAP + within
        slot_rows[k : k + 1, :] = slot
        cols[k] = jnp.transpose(jnp.broadcast_to(slot, (128, count)))
        cols[2 + k] = jnp.transpose(jnp.broadcast_to(weights[k : k + 1, :] / total, (128, count)))

    await_recv(tok.at[pl.ds(0, 3)], tok_rs)

    @pl.loop(0, Z)
    def _(step):
        plane = lax.rem(z + offset_of(step), Z)
        index = (lax.broadcasted_iota(jnp.int32, (PLANE * CAP, count), 0) + plane * (PLANE * CAP)).astype(jnp.float32)
        pick = (index == slot_rows[0:1, :]) | (index == slot_rows[1:2, :])
        moved = jnp.dot(
            jnp.where(pick, 1.0, 0.0).astype(jnp.bfloat16),
            tok[...].reshape(count, 512),
            preferred_element_type=jnp.float32,
        )
        send[pl.ds(plane * PLANE, PLANE)] = moved.reshape(PLANE, CAP, 512).astype(jnp.bfloat16)

        @pl.loop(0, PLANE)
        def _(j):
            target = plane * PLANE + j

            @pl.when(target != ep)
            def _():
                to_ep(send.at[target], rows.at[tp, ep], disp_ss, disp_rs.at[step], target).start()

            @pl.when(target == ep)
            def _():
                rows[tp, ep] = send[ep]

    half = mrows.shape[1] // 2
    await_recv(mrows.at[left], mix_rs.at[0])
    piece = mrows.at[left, pl.ds(0, half)]
    to_tp(piece, piece, mix_ss.at[2], mix_rs.at[2], right).start()
    await_recv(mrows.at[right], mix_rs.at[1])
    piece = mrows.at[right, pl.ds(half, half)]
    to_tp(piece, piece, mix_ss.at[2], mix_rs.at[3], left).start()

    def ring_send(buf, ss, rs, plane, step):
        block = buf.at[tp, pl.ds(plane * PLANE, PLANE)]
        to_tp(block, block, ss.at[0], rs.at[0, step], right).start()
        to_tp(block, block, ss.at[1], rs.at[1, step], left).start()

    def ring_pass(buf, ss, rs, plane, step):
        await_recv(buf.at[left, pl.ds(plane * PLANE, PLANE)], rs.at[0, step])
        block = buf.at[left, pl.ds(plane * PLANE, PLANE // 2)]
        to_tp(block, block, ss.at[2], rs.at[2, step], right).start()
        await_recv(buf.at[right, pl.ds(plane * PLANE, PLANE)], rs.at[1, step])
        block = buf.at[right, pl.ds(plane * PLANE + PLANE // 2, PLANE // 2)]
        to_tp(block, block, ss.at[2], rs.at[3, step], left).start()

    def ring_end(buf, rs, plane, step):
        await_recv(buf.at[far, pl.ds(plane * PLANE, PLANE // 2)], rs.at[2, step])
        await_recv(buf.at[far, pl.ds(plane * PLANE + PLANE // 2, PLANE // 2)], rs.at[3, step])

    def source_plane(step):
        return lax.rem(z + Z - offset_of(step), Z)

    def await_plane(buf, plane, sem, step):
        @pl.when(step == Z - 1)
        def _():
            await_recv(buf.at[pl.ds(plane * PLANE, PLANE - 1)], sem.at[step])

        @pl.when(step != Z - 1)
        def _():
            await_recv(buf.at[pl.ds(plane * PLANE, PLANE)], sem.at[step])

    def stage_rows(step):
        plane = source_plane(step)
        await_plane(rows.at[tp], plane, disp_rs, step)
        ring_send(rows, row_ss, row_rs, plane, step)

    def stage_gate_up(step):
        plane = source_plane(step)
        ring_end(rows, row_rs, plane, step)
        gate = up = None
        for k in range(X):
            x = rows[k, pl.ds(plane * PLANE, PLANE)].reshape(PLANE * CAP, 512)
            g = jnp.dot(x, wg[k * 512 : (k + 1) * 512, :], preferred_element_type=jnp.float32)
            u = jnp.dot(x, wu[k * 512 : (k + 1) * 512, :], preferred_element_type=jnp.float32)
            gate, up = (g, u) if k == 0 else (gate + g, up + u)
        h = gate / (1.0 + jnp.exp(-gate)) * up
        hid[tp, pl.ds(plane * PLANE, PLANE)] = h.reshape(PLANE, CAP, 256).astype(jnp.bfloat16)
        ring_send(hid, hid_ss, hid_rs, plane, step)

    def stage_down(step):
        plane = source_plane(step)
        ring_end(hid, hid_rs, plane, step)
        out = None
        for k in range(X):
            h = hid[k, pl.ds(plane * PLANE, PLANE)].reshape(PLANE * CAP, 256)
            o = jnp.dot(h, wd[k * 256 : (k + 1) * 256, :], preferred_element_type=jnp.float32)
            out = o if k == 0 else out + o
        res[pl.ds(plane * PLANE, PLANE)] = out.reshape(PLANE, CAP, 512).astype(jnp.bfloat16)

        @pl.loop(0, PLANE)
        def _(j):
            target = plane * PLANE + j

            @pl.when(target != ep)
            def _():
                to_ep(res.at[target], ret.at[ep], ret_ss, ret_rs.at[step], target).start()

            @pl.when(target == ep)
            def _():
                ret[ep] = res[ep]

    def stage_combine(step):
        plane = lax.rem(z + offset_of(step), Z)
        await_plane(ret, plane, ret_rs, step)
        index = lax.broadcasted_iota(jnp.int32, (count, PLANE * CAP), 1) + plane * (PLANE * CAP)
        index = index.astype(jnp.float32)
        share = jnp.where(cols[0][:, 0:1] == index, cols[2][:, 0:1], 0.0)
        share = jnp.where(cols[1][:, 0:1] == index, cols[3][:, 0:1], share)
        high = share.astype(jnp.bfloat16)
        low = (share - high.astype(jnp.float32)).astype(jnp.bfloat16)
        got = ret[pl.ds(plane * PLANE, PLANE)].reshape(PLANE * CAP, 512)
        acc[...] += jnp.dot(high, got, preferred_element_type=jnp.float32) + jnp.dot(
            low, got, preferred_element_type=jnp.float32
        )

    acc[...] = jnp.zeros(acc.shape, jnp.float32)
    for load in loads[:3]:
        load.wait()
    stage_rows(0)
    stage_rows(1)

    await_recv(mrows.at[far, pl.ds(0, half)], mix_rs.at[2])
    await_recv(mrows.at[far, pl.ds(half, half)], mix_rs.at[3])

    @pl.loop(0, 2)
    def _(n):
        span = pl.ds(pl.multiple_of(n * 256, 256), 256)
        m = mrows[...].reshape(count, 2048)
        in_gate = jnp.dot(m, wi[:, span], preferred_element_type=jnp.float32)
        values = jnp.dot(m, wv[:, span], preferred_element_type=jnp.float32)
        product = (in_gate * values).astype(jnp.bfloat16)
        ext[8:, span] = product.astype(jnp.float32)
        rim_s[:, span] = product[count - 16 :]
        ogate[:, span] = jnp.dot(m, wo[:, span], preferred_element_type=jnp.float32)

    to_ep(rim_s, rim_r, rim_ss, rim_rs, lax.rem(ep + 1, EP)).start()
    for load in loads[3:]:
        load.wait()

    def stage_gated():
        await_recv(rim_r, rim_rs)
        before = rim_r[...].astype(jnp.float32)[8:]
        ext[0:8, :] = jnp.where(ep == 0, jnp.zeros_like(before), before)

        @pl.loop(0, 4)
        def _(n):
            span = pl.ds(pl.multiple_of(n * 128, 128), 128)
            tap_span = pl.ds(pl.multiple_of(tp * 512 + n * 128, 128), 128)
            conv = taps[0:1, tap_span] * ext[6 : 6 + count, span]
            conv = conv + taps[1:2, tap_span] * ext[7 : 7 + count, span]
            conv = conv + taps[2:3, tap_span] * ext[8 : 8 + count, span]
            gat[tp, :, span] = (ogate[:, span] * conv).astype(jnp.bfloat16)

    @pl.loop(2, Z + 5)
    def _(s):
        @pl.when(s < Z)
        def _():
            stage_rows(s)

        @pl.when(s < Z + 2)
        def _():
            ring_pass(rows, row_ss, row_rs, source_plane(s - 2), s - 2)

        @pl.when((s >= 3) & (s < Z + 3))
        def _():
            stage_gate_up(s - 3)

        @pl.when((s >= 4) & (s < Z + 4))
        def _():
            ring_pass(hid, hid_ss, hid_rs, source_plane(s - 4), s - 4)

        @pl.when(s >= 5)
        def _():
            stage_down(s - 5)

        @pl.when(s == 4)
        def _():
            stage_gated()

        @pl.when(s == Z + 3)
        def _():
            to_tp(gat.at[tp], gat.at[tp], gat_ss.at[0], gat_rs.at[0], right).start()
            to_tp(gat.at[tp], gat.at[tp], gat_ss.at[1], gat_rs.at[1], left).start()

        @pl.when(s >= 7)
        def _():
            stage_combine(s - 7)

    half_g = count // 2
    await_recv(gat.at[left], gat_rs.at[0])
    piece = gat.at[left, pl.ds(0, half_g)]
    to_tp(piece, piece, gat_ss.at[2], gat_rs.at[2], right).start()
    await_recv(gat.at[right], gat_rs.at[1])
    piece = gat.at[right, pl.ds(half_g, half_g)]
    to_tp(piece, piece, gat_ss.at[2], gat_rs.at[3], left).start()
    stage_combine(Z - 2)
    stage_combine(Z - 1)
    expert_out[...] = acc[...].astype(jnp.bfloat16)
    await_recv(gat.at[far, pl.ds(0, half_g)], gat_rs.at[2])
    await_recv(gat.at[far, pl.ds(half_g, half_g)], gat_rs.at[3])

    @pl.loop(0, 2)
    def _(n):
        span = pl.ds(pl.multiple_of(n * 256, 256), 256)
        out = None
        for k in range(X):
            o = jnp.dot(gat[k], wp[k * 512 : (k + 1) * 512, span], preferred_element_type=jnp.float32)
            out = o if k == 0 else out + o
        mixer_out[:, span] = out.astype(jnp.bfloat16)

    await_send(tok.at[pl.ds(0, 3)], tok_ss)
    await_send(send.at[pl.ds(0, EP - 1)], disp_ss)
    await_send(res.at[pl.ds(0, EP - 1)], ret_ss)
    await_send(rim_s, rim_ss)
    for buf, sem in ((mrows, mix_ss), (rows, row_ss), (hid, hid_ss), (gat, gat_ss)):
        for i in range(3):
            await_send(buf.at[0], sem.at[i])


def on_device(
    mixer_in, expert_in, mixer_gain, in_gate_weight, out_gate_weight, value_weight, conv_taps, mixer_proj,
    expert_gain, route_ids, route_weights, gate_weight, up_weight, down_weight,
):
    bf16, f32 = jnp.bfloat16, jnp.float32
    own, wide = mixer_in.shape
    count = route_ids.shape[0]
    local = pl.BlockSpec(memory_space=pltpu.VMEM)
    remote = pl.BlockSpec(memory_space=pl.ANY)
    dma, vmem = pltpu.SemaphoreType.DMA, pltpu.VMEM
    out = jax.ShapeDtypeStruct((count, 512), bf16)
    return pl.pallas_call(
        kernel,
        out_shape=(out, out),
        in_specs=[local] * 7 + [remote] * 7,
        out_specs=(local, local),
        scratch_shapes=[
            *[vmem((wide, 512), bf16)] * 4, *[vmem((wide, 256), bf16)] * 2, vmem((1024, 512), bf16),
            vmem((X, own, 512), bf16), vmem((X, own, 512), bf16), vmem((X, own, wide), bf16),
            vmem((EP, CAP, 512), bf16), vmem((X, EP, CAP, 512), bf16), vmem((X, EP, CAP, 256), bf16),
            vmem((EP, CAP, 512), bf16), vmem((EP, CAP, 512), bf16), vmem((X, count, 512), bf16),
            vmem((count + 8, 512), f32), vmem((count, 512), f32), vmem((count, 512), f32),
            vmem((16, 512), bf16), vmem((16, 512), bf16), vmem((8, count), f32), vmem((4, count, 128), f32),
            dma((7,)), dma, dma, dma((3,)), dma((4,)), dma, dma((Z,)), dma((3,)), dma((4, Z)), dma((3,)), dma((4, Z)),
            dma, dma((Z,)), dma((3,)), dma((4,)), dma, dma,
        ],
        compiler_params=pltpu.CompilerParams(
            collective_id=0, has_side_effects=True, vmem_limit_bytes=62 * 2**20
        ),
        name="mixer_and_experts",
    )(
        mixer_in, expert_in, mixer_gain.reshape(1, -1), expert_gain.reshape(1, -1), conv_taps,
        route_ids.T, route_weights.T,
        in_gate_weight, out_gate_weight, value_weight, mixer_proj, gate_weight[0], up_weight[0], down_weight[0],
    )


def solution(mesh):
    return jax.shard_map(
        on_device,
        mesh=mesh,
        in_specs=(
            P(("ep", "tp"), None),
            P(("ep", "tp"), None),
            P(),
            P(None, "tp"),
            P(None, "tp"),
            P(None, "tp"),
            P(),
            P(None, "tp"),
            P(),
            P("ep", None),
            P("ep", None),
            P("ep", None, "tp"),
            P("ep", None, "tp"),
            P("ep", None, "tp"),
        ),
        out_specs=(P("ep", "tp"), P("ep", "tp")),
        check_vma=False,
    )
```

```python
import jax
import jax.numpy as jnp
from jax import lax
from jax.experimental import pallas as pl
from jax.experimental.pallas import tpu as pltpu
from jax.sharding import PartitionSpec as P

norm_eps = 1e-06
Z, Y, C, X = 8, 4, 2, 4
PLANE = Y * C
EP = Z * PLANE
CAP = 24
ORDER = (2, 6, 3, 5, 4, 1, 7, 0)
LAG = 10
FAR = 5
MESH = pl.DeviceIdType.MESH


def rms_rows(values, gain_row):
    wide = values.astype(jnp.float32)
    scale = lax.rsqrt(jnp.mean(wide * wide, axis=-1, keepdims=True) + norm_eps)
    return (wide * scale * gain_row).astype(jnp.bfloat16)


def offset_of(step):
    dz = 0
    for at, offset in enumerate(ORDER):
        dz = jnp.where(step == at, offset, dz)
    return dz


def kernel(
    mixer_in, expert_in, mixer_gain, expert_gain, taps, ids, weights,
    wi_hbm, wo_hbm, wv_hbm, wp_hbm, wg_hbm, wu_hbm, wd_hbm,
    mixer_out, expert_out,
    wi, wo, wv, wp, wg, wu, wd,
    tok, mrows, send, near, rows, hid, res, ret, gat, ext, ogate, acc, rim_s, rim_r, slot_rows, cols,
    load_sem, tok_ss, tok_rs, mix_ss, mix_rs, disp_ss, near_ss, disp_rs, row_ss, row_rs, hid_ss, hid_rs,
    ret_ss, ret_rs, gat_ss, gat_rs, rim_ss, rim_rs,
):
    ep, tp = lax.axis_index("ep"), lax.axis_index("tp")
    z = ep // PLANE
    right, left, far = lax.rem(tp + 1, X), lax.rem(tp + 3, X), lax.rem(tp + 2, X)

    loads = [
        pltpu.make_async_copy(src, dst, load_sem.at[i])
        for i, (src, dst) in enumerate(
            ((wi_hbm, wi), (wo_hbm, wo), (wv_hbm, wv), (wg_hbm, wg), (wu_hbm, wu), (wd_hbm, wd), (wp_hbm, wp))
        )
    ]
    for load in loads:
        load.start()

    barrier = pltpu.get_barrier_semaphore()

    @pl.loop(1, EP)
    def _(d):
        pl.semaphore_signal(barrier, inc=1, device_id={"ep": lax.rem(ep + d, EP)}, device_id_type=MESH)

    for other in (right, left, far):
        pl.semaphore_signal(barrier, inc=1, device_id={"tp": other}, device_id_type=MESH)

    def to_ep(src, dst, ss, rs, target):
        return pltpu.make_async_remote_copy(src, dst, ss, rs, device_id={"ep": target}, device_id_type=MESH)

    def to_tp(src, dst, ss, rs, target):
        return pltpu.make_async_remote_copy(src, dst, ss, rs, device_id={"tp": target}, device_id_type=MESH)

    def await_recv(ref, sem):
        to_tp(ref, ref, sem, sem, right).wait_recv()

    def await_send(ref, sem):
        to_tp(ref, ref, sem, sem, right).wait_send()

    normed = rms_rows(expert_in[...], expert_gain[...])
    for k in range(X):
        tok[tp, k] = normed[:, k * 512 : (k + 1) * 512]
    mrows[tp] = rms_rows(mixer_in[...], mixer_gain[...])

    pl.semaphore_wait(barrier, EP + 2)

    for i in range(X):
        k = lax.rem(tp + 1 + i, X)
        to_tp(tok.at[tp, k], tok.at[tp, k], tok_ss.at[0], tok_rs.at[0, i], right).start()
        k = lax.rem(tp + 2 * X - 1 - i, X)
        to_tp(tok.at[tp, k], tok.at[tp, k], tok_ss.at[1], tok_rs.at[1, i], left).start()

    count = ids.shape[1]
    labels = lax.broadcasted_iota(jnp.int32, (EP, count), 0)
    hot = [ids[k : k + 1, :] == labels for k in range(2)]
    named = jnp.where(hot[0] | hot[1], 1.0, 0.0).astype(jnp.bfloat16)
    older = (
        lax.broadcasted_iota(jnp.int32, (count, count), 0) < lax.broadcasted_iota(jnp.int32, (count, count), 1)
    )
    earlier = jnp.dot(named, jnp.where(older, 1.0, 0.0).astype(jnp.bfloat16), preferred_element_type=jnp.float32)
    total = weights[0:1, :] + weights[1:2, :]
    for k in range(2):
        within = jnp.sum(jnp.where(hot[k], earlier, 0.0), axis=0, keepdims=True)
        slot = ids[k : k + 1, :].astype(jnp.float32) * CAP + within
        slot_rows[k : k + 1, :] = slot
        cols[k] = jnp.transpose(jnp.broadcast_to(slot, (128, count)))
        cols[2 + k] = jnp.transpose(jnp.broadcast_to(weights[k : k + 1, :] / total, (128, count)))

    def token_pass(side, i, other, source):
        k = lax.rem(tp + i, X) if side == 0 else lax.rem(tp + X - i, X)
        await_recv(tok.at[source, k], tok_rs.at[side, i])
        if i in ((1, 2) if side == 0 else (2, 3)):
            piece = tok.at[source, k]
            to_tp(piece, piece, tok_ss.at[2], tok_rs.at[2 + side, i], other).start()

    token_pass(0, 0, right, left)
    token_pass(0, 1, right, left)
    token_pass(1, 0, left, right)
    to_tp(mrows.at[tp], mrows.at[tp], mix_ss.at[0], mix_rs.at[0], right).start()
    to_tp(mrows.at[tp], mrows.at[tp], mix_ss.at[1], mix_rs.at[1], left).start()
    await_recv(tok.at[far, tp], tok_rs.at[2, 1])

    @pl.loop(0, FAR)
    def _(step):
        plane = lax.rem(z + offset_of(step), Z)
        index = (lax.broadcasted_iota(jnp.int32, (PLANE * CAP, count), 0) + plane * (PLANE * CAP)).astype(jnp.float32)
        pick = (index == slot_rows[0:1, :]) | (index == slot_rows[1:2, :])
        moved = jnp.dot(
            jnp.where(pick, 1.0, 0.0).astype(jnp.bfloat16),
            tok[:, tp].reshape(count, 512),
            preferred_element_type=jnp.float32,
        )
        send[pl.ds(plane * PLANE, PLANE)] = moved.reshape(PLANE, CAP, 512).astype(jnp.bfloat16)

        @pl.loop(0, PLANE)
        def _(j):
            target = plane * PLANE + j

            to_ep(send.at[target], rows.at[tp, ep], disp_ss, disp_rs.at[step], target).start()

    token_pass(0, 2, right, left)
    token_pass(0, 3, right, left)
    for i in range(1, X):
        token_pass(1, i, left, right)

    half = mrows.shape[1] // 2
    await_recv(mrows.at[left], mix_rs.at[0])
    piece = mrows.at[left, pl.ds(0, half)]
    to_tp(piece, piece, mix_ss.at[2], mix_rs.at[2], right).start()
    await_recv(mrows.at[right], mix_rs.at[1])
    piece = mrows.at[right, pl.ds(half, half)]
    to_tp(piece, piece, mix_ss.at[2], mix_rs.at[3], left).start()

    await_recv(tok.at[far, lax.rem(tp + 1, X)], tok_rs.at[2, 2])
    await_recv(tok.at[far, lax.rem(tp + 3, X)], tok_rs.at[3, 2])
    await_recv(tok.at[far, lax.rem(tp + 2, X)], tok_rs.at[3, 3])

    @pl.loop(FAR, Z)
    def _(step):
        plane = lax.rem(z + offset_of(step), Z)
        index = (lax.broadcasted_iota(jnp.int32, (PLANE * CAP, count), 0) + plane * (PLANE * CAP)).astype(jnp.float32)
        pick = (index == slot_rows[0:1, :]) | (index == slot_rows[1:2, :])
        pick = jnp.where(pick, 1.0, 0.0).astype(jnp.bfloat16)
        first = (step - FAR) * PLANE
        for k in range(X):
            moved = jnp.dot(pick, tok[:, k].reshape(count, 512), preferred_element_type=jnp.float32)
            near[pl.ds(first, PLANE), k] = moved.reshape(PLANE, CAP, 512).astype(jnp.bfloat16)

        @pl.loop(0, PLANE)
        def _(j):
            target = plane * PLANE + j

            @pl.when(target != ep)
            def _():
                to_ep(near.at[first + j], rows.at[:, ep], near_ss, disp_rs.at[step], target).start()

            @pl.when(target == ep)
            def _():
                for k in range(X):
                    rows[k, ep] = near[first + j, k]

    def ring_send(buf, ss, rs, plane, step):
        block = buf.at[tp, pl.ds(plane * PLANE, PLANE)]
        to_tp(block, block, ss.at[0], rs.at[0, step], right).start()
        to_tp(block, block, ss.at[1], rs.at[1, step], left).start()

    def ring_pass(buf, ss, rs, plane, step):
        await_recv(buf.at[left, pl.ds(plane * PLANE, PLANE)], rs.at[0, step])
        block = buf.at[left, pl.ds(plane * PLANE, PLANE // 2)]
        to_tp(block, block, ss.at[2], rs.at[2, step], right).start()
        await_recv(buf.at[right, pl.ds(plane * PLANE, PLANE)], rs.at[1, step])
        block = buf.at[right, pl.ds(plane * PLANE + PLANE // 2, PLANE // 2)]
        to_tp(block, block, ss.at[2], rs.at[3, step], left).start()

    def ring_end(buf, rs, plane, step):
        await_recv(buf.at[far, pl.ds(plane * PLANE, PLANE // 2)], rs.at[2, step])
        await_recv(buf.at[far, pl.ds(plane * PLANE + PLANE // 2, PLANE // 2)], rs.at[3, step])

    def source_plane(step):
        return lax.rem(z + Z - offset_of(step), Z)

    def await_plane(buf, plane, sem, step):
        @pl.when(step == Z - 1)
        def _():
            await_recv(buf.at[pl.ds(plane * PLANE, PLANE - 1)], sem.at[step])

        @pl.when(step != Z - 1)
        def _():
            await_recv(buf.at[pl.ds(plane * PLANE, PLANE)], sem.at[step])

    def stage_rows(step):
        plane = source_plane(step)
        await_recv(rows.at[tp, pl.ds(plane * PLANE, PLANE)], disp_rs.at[step])
        ring_send(rows, row_ss, row_rs, plane, step)

    def stage_gate_up(step):
        plane = source_plane(step)

        @pl.when(step < FAR)
        def _():
            ring_end(rows, row_rs, plane, step)

        @pl.when((step >= FAR) & (step < Z - 1))
        def _():
            await_recv(rows.at[:, pl.ds(plane * PLANE, PLANE)], disp_rs.at[step])

        @pl.when(step == Z - 1)
        def _():
            await_recv(rows.at[:, pl.ds(plane * PLANE, PLANE - 1)], disp_rs.at[step])

        gate = up = None
        for k in range(X):
            x = rows[k, pl.ds(plane * PLANE, PLANE)].reshape(PLANE * CAP, 512)
            g = jnp.dot(x, wg[k * 512 : (k + 1) * 512, :], preferred_element_type=jnp.float32)
            u = jnp.dot(x, wu[k * 512 : (k + 1) * 512, :], preferred_element_type=jnp.float32)
            gate, up = (g, u) if k == 0 else (gate + g, up + u)
        h = gate / (1.0 + jnp.exp(-gate)) * up
        hid[tp, pl.ds(plane * PLANE, PLANE)] = h.reshape(PLANE, CAP, 256).astype(jnp.bfloat16)
        ring_send(hid, hid_ss, hid_rs, plane, step)

    def stage_down(step):
        plane = source_plane(step)
        ring_end(hid, hid_rs, plane, step)
        out = None
        for k in range(X):
            h = hid[k, pl.ds(plane * PLANE, PLANE)].reshape(PLANE * CAP, 256)
            o = jnp.dot(h, wd[k * 256 : (k + 1) * 256, :], preferred_element_type=jnp.float32)
            out = o if k == 0 else out + o
        res[pl.ds(plane * PLANE, PLANE)] = out.reshape(PLANE, CAP, 512).astype(jnp.bfloat16)

        @pl.loop(0, PLANE)
        def _(j):
            target = plane * PLANE + j

            @pl.when(target != ep)
            def _():
                to_ep(res.at[target], ret.at[ep], ret_ss, ret_rs.at[step], target).start()

            @pl.when(target == ep)
            def _():
                ret[ep] = res[ep]

    def stage_combine(step):
        plane = lax.rem(z + offset_of(step), Z)
        await_plane(ret, plane, ret_rs, step)
        index = lax.broadcasted_iota(jnp.int32, (count, PLANE * CAP), 1) + plane * (PLANE * CAP)
        index = index.astype(jnp.float32)
        share = jnp.where(cols[0][:, 0:1] == index, cols[2][:, 0:1], 0.0)
        share = jnp.where(cols[1][:, 0:1] == index, cols[3][:, 0:1], share)
        high = share.astype(jnp.bfloat16)
        low = (share - high.astype(jnp.float32)).astype(jnp.bfloat16)
        got = ret[pl.ds(plane * PLANE, PLANE)].reshape(PLANE * CAP, 512)
        acc[...] += jnp.dot(high, got, preferred_element_type=jnp.float32) + jnp.dot(
            low, got, preferred_element_type=jnp.float32
        )

    acc[...] = jnp.zeros(acc.shape, jnp.float32)
    for load in loads[:3]:
        load.wait()
    stage_rows(0)
    stage_rows(1)

    await_recv(mrows.at[far, pl.ds(0, half)], mix_rs.at[2])
    await_recv(mrows.at[far, pl.ds(half, half)], mix_rs.at[3])

    @pl.loop(0, 2)
    def _(n):
        span = pl.ds(pl.multiple_of(n * 256, 256), 256)
        m = mrows[...].reshape(count, 2048)
        in_gate = jnp.dot(m, wi[:, span], preferred_element_type=jnp.float32)
        values = jnp.dot(m, wv[:, span], preferred_element_type=jnp.float32)
        product = (in_gate * values).astype(jnp.bfloat16)
        ext[8:, span] = product.astype(jnp.float32)
        rim_s[:, span] = product[count - 16 :]
        ogate[:, span] = jnp.dot(m, wo[:, span], preferred_element_type=jnp.float32)

    to_ep(rim_s, rim_r, rim_ss, rim_rs, lax.rem(ep + 1, EP)).start()
    for load in loads[3:]:
        load.wait()

    def stage_gated():
        await_recv(rim_r, rim_rs)
        before = rim_r[...].astype(jnp.float32)[8:]
        ext[0:8, :] = jnp.where(ep == 0, jnp.zeros_like(before), before)

        @pl.loop(0, 4)
        def _(n):
            span = pl.ds(pl.multiple_of(n * 128, 128), 128)
            tap_span = pl.ds(pl.multiple_of(tp * 512 + n * 128, 128), 128)
            conv = taps[0:1, tap_span] * ext[6 : 6 + count, span]
            conv = conv + taps[1:2, tap_span] * ext[7 : 7 + count, span]
            conv = conv + taps[2:3, tap_span] * ext[8 : 8 + count, span]
            gat[tp, :, span] = (ogate[:, span] * conv).astype(jnp.bfloat16)

    @pl.loop(2, Z + 5)
    def _(s):
        @pl.when(s < FAR)
        def _():
            stage_rows(s)

        @pl.when(s < FAR + 2)
        def _():
            ring_pass(rows, row_ss, row_rs, source_plane(s - 2), s - 2)

        @pl.when((s >= 3) & (s < Z + 3))
        def _():
            stage_gate_up(s - 3)

        @pl.when((s >= 4) & (s < Z + 4))
        def _():
            ring_pass(hid, hid_ss, hid_rs, source_plane(s - 4), s - 4)

        @pl.when(s >= 5)
        def _():
            stage_down(s - 5)

        @pl.when(s == 4)
        def _():
            stage_gated()

        @pl.when(s == Z + 3)
        def _():
            to_tp(gat.at[tp], gat.at[tp], gat_ss.at[0], gat_rs.at[0], right).start()
            to_tp(gat.at[tp], gat.at[tp], gat_ss.at[1], gat_rs.at[1], left).start()

        @pl.when(s >= LAG)
        def _():
            stage_combine(s - LAG)

    half_g = count // 2
    await_recv(gat.at[left], gat_rs.at[0])
    piece = gat.at[left, pl.ds(0, half_g)]
    to_tp(piece, piece, gat_ss.at[2], gat_rs.at[2], right).start()
    await_recv(gat.at[right], gat_rs.at[1])
    piece = gat.at[right, pl.ds(half_g, half_g)]
    to_tp(piece, piece, gat_ss.at[2], gat_rs.at[3], left).start()

    @pl.loop(Z + 5 - LAG, Z)
    def _(step):
        stage_combine(step)

    expert_out[...] = acc[...].astype(jnp.bfloat16)
    await_recv(gat.at[far, pl.ds(0, half_g)], gat_rs.at[2])
    await_recv(gat.at[far, pl.ds(half_g, half_g)], gat_rs.at[3])

    @pl.loop(0, 2)
    def _(n):
        span = pl.ds(pl.multiple_of(n * 256, 256), 256)
        out = None
        for k in range(X):
            o = jnp.dot(gat[k], wp[k * 512 : (k + 1) * 512, span], preferred_element_type=jnp.float32)
            out = o if k == 0 else out + o
        mixer_out[:, span] = out.astype(jnp.bfloat16)

    await_send(send.at[pl.ds(0, FAR * PLANE)], disp_ss)
    await_send(near.at[pl.ds(0, (Z - FAR) * PLANE - 1)], near_ss)
    await_send(res.at[pl.ds(0, EP - 1)], ret_ss)
    await_send(rim_s, rim_ss)
    for buf, sem in ((tok, tok_ss), (mrows, mix_ss), (hid, hid_ss), (gat, gat_ss)):
        for i in range(3):
            await_send(buf.at[0], sem.at[i])
    for i in range(3):
        await_send(rows.at[0, pl.ds(0, FAR * PLANE)], row_ss.at[i])


def hand_over(mixer_in, expert_in, mixer_out, expert_out, held, in_sem, out_sem):
    ins = [pltpu.make_async_copy(src, held.at[i], in_sem.at[i]) for i, src in enumerate((mixer_in, expert_in))]
    outs = [pltpu.make_async_copy(held.at[i], dst, out_sem.at[i]) for i, dst in enumerate((mixer_out, expert_out))]
    for copy in ins:
        copy.start()
    for i in range(2):
        ins[i].wait()
        outs[i].start()
    for copy in outs:
        copy.wait()


def on_device(
    mixer_in, expert_in, mixer_gain, in_gate_weight, out_gate_weight, value_weight, conv_taps, mixer_proj,
    expert_gain, route_ids, route_weights, gate_weight, up_weight, down_weight,
):
    bf16, f32 = jnp.bfloat16, jnp.float32
    own, wide = mixer_in.shape
    count = route_ids.shape[0]
    local = pl.BlockSpec(memory_space=pltpu.VMEM)
    remote = pl.BlockSpec(memory_space=pl.ANY)
    dma, vmem = pltpu.SemaphoreType.DMA, pltpu.VMEM
    out = jax.ShapeDtypeStruct((count, 512), bf16)
    results = pl.pallas_call(
        kernel,
        out_shape=(out, out),
        in_specs=[local] * 7 + [remote] * 7,
        out_specs=(local, local),
        scratch_shapes=[
            *[vmem((wide, 512), bf16)] * 4, *[vmem((wide, 256), bf16)] * 2, vmem((1024, 512), bf16),
            vmem((X, X, own, 512), bf16), vmem((X, own, wide), bf16),
            vmem((EP, CAP, 512), bf16), vmem(((Z - FAR) * PLANE, X, CAP, 512), bf16), vmem((X, EP, CAP, 512), bf16), vmem((X, EP, CAP, 256), bf16),
            vmem((EP, CAP, 512), bf16), vmem((EP, CAP, 512), bf16), vmem((X, count, 512), bf16),
            vmem((count + 8, 512), f32), vmem((count, 512), f32), vmem((count, 512), f32),
            vmem((16, 512), bf16), vmem((16, 512), bf16), vmem((8, count), f32), vmem((4, count, 128), f32),
            dma((7,)), dma((3,)), dma((4, X)), dma((3,)), dma((4,)), dma, dma, dma((Z,)), dma((3,)), dma((4, Z)), dma((3,)), dma((4, Z)),
            dma, dma((Z,)), dma((3,)), dma((4,)), dma, dma,
        ],
        compiler_params=pltpu.CompilerParams(
            collective_id=0, has_side_effects=True, vmem_limit_bytes=62 * 2**20
        ),
        name="mixer_and_experts",
    )(
        mixer_in, expert_in, mixer_gain.reshape(1, -1), expert_gain.reshape(1, -1), conv_taps,
        route_ids.T, route_weights.T,
        in_gate_weight, out_gate_weight, value_weight, mixer_proj, gate_weight[0], up_weight[0], down_weight[0],
    )
    return pl.pallas_call(
        hand_over,
        out_shape=(out, out),
        in_specs=[remote] * 2,
        out_specs=(remote, remote),
        scratch_shapes=[vmem((2, count, 512), bf16), dma((2,)), dma((2,))],
        name="hand_over",
    )(*results)


def solution(mesh):
    return jax.shard_map(
        on_device,
        mesh=mesh,
        in_specs=(
            P(("ep", "tp"), None),
            P(("ep", "tp"), None),
            P(),
            P(None, "tp"),
            P(None, "tp"),
            P(None, "tp"),
            P(),
            P(None, "tp"),
            P(),
            P("ep", None),
            P("ep", None),
            P("ep", None, "tp"),
            P("ep", None, "tp"),
            P("ep", None, "tp"),
        ),
        out_specs=(P("ep", "tp"), P("ep", "tp")),
        check_vma=False,
    )
```

```python
import jax
import jax.numpy as jnp
from jax import lax
from jax.experimental import pallas as pl
from jax.experimental.pallas import tpu as pltpu
from jax.sharding import PartitionSpec as P

norm_eps = 1e-06
Z, Y, C, X = 8, 4, 2, 4
PLANE = Y * C
EP = Z * PLANE
CHIPS = Z * Y
CAP = 24
SEND = (0, 1, 7, 2, 6, 3, 5, 4)
BACK = (4, 3, 5, 2, 6, 1, 7, 0)
PAIR, DOWN = 6, 8
MESH = pl.DeviceIdType.MESH


def pick_of(table, step):
    value = table[0]
    for at in range(1, len(table)):
        value = jnp.where(step == at, table[at], value)
    return value


def rms_rows(values, gain_row):
    wide = values.astype(jnp.float32)
    scale = lax.rsqrt(jnp.mean(wide * wide, axis=-1, keepdims=True) + norm_eps)
    return (wide * scale * gain_row).astype(jnp.bfloat16)


def kernel(
    mixer_in, expert_in, mixer_gain, expert_gain, taps, ids, weights,
    wi_hbm, wo_hbm, wv_hbm, wp_hbm, wg_hbm, wu_hbm, wd_hbm,
    mixer_out, expert_out,
    wi, wo, wv, wp, wg, wu, wd,
    route, tok_send, tok, mrows, send, rows, hid, res, ret, gat, ext, ogate, acc, rim_s, rim_r, slot_rows, cols,
    fin, fin_same, fin_pair,
    load_sem, wt_ss, wt_rs, route_ss, route_rs, tok_ss, tok_rs, mix_ss, mix_rs, disp_ss, disp_rs, row_ss, row_rs,
    hid_ss, hid_rs, ret_ss, ret_rs, gat_ss, gat_rs, rim_ss, rim_rs, fin_ss, fin_rs,
):
    ep, tp = lax.axis_index("ep"), lax.axis_index("tp")
    z, core = ep // PLANE, lax.rem(ep, C)
    chip, twin = ep // C, ep + 1 - 2 * core
    odd = lax.rem(tp, 2)
    pair = tp + 1 - 2 * odd
    mate = lax.rem(tp + 3 + 2 * odd, X)
    far = lax.rem(tp + 2, X)
    u = 1 - odd
    first = lax.rem(tp + X - u, X)
    count = ids.shape[1]

    loads = [
        pltpu.make_async_copy(src, dst, load_sem.at[i])
        for i, (src, dst) in enumerate(
            ((wg_hbm, wg.at[0]), (wu_hbm, wu.at[0]), (wd_hbm, wd.at[0]),
             (wi_hbm, wi), (wo_hbm, wo), (wv_hbm, wv), (wp_hbm, wp))
        )
    ]
    for load in loads:
        load.start()

    barrier = pltpu.get_barrier_semaphore()

    @pl.loop(1, EP)
    def _(d):
        pl.semaphore_signal(barrier, inc=1, device_id={"ep": lax.rem(ep + d, EP)}, device_id_type=MESH)

    for other in (pair, mate):
        pl.semaphore_signal(barrier, inc=1, device_id={"tp": other}, device_id_type=MESH)
        pl.semaphore_signal(barrier, inc=1, device_id={"ep": twin, "tp": other}, device_id_type=MESH)

    def to_ep(src, dst, ss, rs, target):
        return pltpu.make_async_remote_copy(src, dst, ss, rs, device_id={"ep": target}, device_id_type=MESH)

    def to_tp(src, dst, ss, rs, target):
        return pltpu.make_async_remote_copy(src, dst, ss, rs, device_id={"tp": target}, device_id_type=MESH)

    def to_twin(src, dst, ss, rs, target):
        return pltpu.make_async_remote_copy(
            src, dst, ss, rs, device_id={"ep": twin, "tp": target}, device_id_type=MESH
        )

    def await_recv(ref, sem):
        to_tp(ref, ref, sem, sem, mate).wait_recv()

    def await_send(ref, sem):
        to_tp(ref, ref, sem, sem, mate).wait_send()

    picks = jnp.concatenate(
        [ids[...].astype(jnp.float32), weights[...], jnp.zeros((4, count), jnp.float32)], axis=0
    )
    turned = jnp.where((first == 1) == (core == 0), pltpu.roll(picks, 3 * count // 4, 1), pltpu.roll(picks, count // 4, 1))
    route[core] = turned
    normed = rms_rows(expert_in[...], expert_gain[...])
    for k in range(X):
        tok_send[k] = normed[:, k * 512 : (k + 1) * 512]
    tok[core, u] = tok_send[2 * u + core]
    mrows[tp] = rms_rows(mixer_in[...], mixer_gain[...])

    for load in loads[:3]:
        load.wait()
    pl.semaphore_wait(barrier, EP + 3)

    to_ep(route.at[core], route.at[core], route_ss, route_rs, twin).start()
    to_twin(tok_send.at[2 * (1 - u) + 1 - core], tok.at[core, u], tok_ss, tok_rs, mate).start()
    to_tp(tok_send.at[2 * (1 - u) + core], tok.at[core, u], tok_ss, tok_rs, mate).start()
    to_ep(tok_send.at[2 * u + 1 - core], tok.at[core, u], tok_ss, tok_rs, twin).start()
    to_tp(wg.at[0], wg.at[1], wt_ss.at[0], wt_rs.at[0], pair).start()
    to_tp(wu.at[0], wu.at[1], wt_ss.at[1], wt_rs.at[1], pair).start()
    to_tp(mrows.at[tp], mrows.at[tp], mix_ss.at[0], mix_rs.at[0], pair).start()
    to_tp(wd.at[0], wd.at[1], wt_ss.at[2], wt_rs.at[2], pair).start()

    await_recv(route.at[1 - core], route_rs)
    lane = lax.broadcasted_iota(jnp.int32, (8, count), 1)
    both = jnp.where(lane < count // 2, route[0], route[1])
    labels = lax.broadcasted_iota(jnp.int32, (EP, count), 0).astype(jnp.float32)
    hot = [both[k : k + 1, :] == labels for k in range(2)]
    named = jnp.where(hot[0] | hot[1], 1.0, 0.0).astype(jnp.bfloat16)
    older = (
        lax.broadcasted_iota(jnp.int32, (count, count), 0) < lax.broadcasted_iota(jnp.int32, (count, count), 1)
    )
    earlier = jnp.dot(named, jnp.where(older, 1.0, 0.0).astype(jnp.bfloat16), preferred_element_type=jnp.float32)
    total = both[2:3, :] + both[3:4, :]
    for k in range(2):
        within = jnp.sum(jnp.where(hot[k], earlier, 0.0), axis=0, keepdims=True)
        slot = both[k : k + 1, :] * CAP + within
        slot_rows[k : k + 1, :] = slot
        cols[k] = jnp.transpose(jnp.broadcast_to(slot, (128, count)))
        cols[2 + k] = jnp.transpose(jnp.broadcast_to(both[2 + k : 3 + k, :] / total, (128, count)))

    await_recv(send.at[pl.ds(0, 12)], tok_rs)
    to_tp(mrows.at[tp], mrows.at[tp], mix_ss.at[1], mix_rs.at[1], mate).start()

    @pl.loop(0, Z)
    def _(step):
        plane = lax.rem(z + pick_of(SEND, step), Z)
        index = (lax.broadcasted_iota(jnp.int32, (PLANE * CAP, count), 0) + plane * (PLANE * CAP)).astype(jnp.float32)
        pick = (index == slot_rows[0:1, :]) | (index == slot_rows[1:2, :])
        moved = jnp.dot(
            jnp.where(pick, 1.0, 0.0).astype(jnp.bfloat16),
            tok[...].reshape(count, 512),
            preferred_element_type=jnp.float32,
        )
        send[pl.ds(plane * PLANE, PLANE)] = moved.reshape(PLANE, CAP, 512).astype(jnp.bfloat16)

        @pl.loop(0, PLANE)
        def _(j):
            target = plane * PLANE + j

            @pl.when(target != ep)
            def _():
                to_ep(send.at[target], rows.at[2 * u + core, chip], disp_ss, disp_rs.at[step], target).start()

            @pl.when(target == ep)
            def _():
                rows[2 * u + core, chip] = send[ep]

    def source_chips(offset):
        return pl.ds(lax.rem(z + Z - offset, Z) * Y, Y)

    def await_slabs(sem, last):
        @pl.when(last)
        def _():
            await_recv(send.at[pl.ds(0, PLANE - 1)], sem)

        @pl.when(jnp.logical_not(last))
        def _():
            await_recv(send.at[pl.ds(0, PLANE)], sem)

    def stage_rows(step):
        block = rows.at[pl.ds(2 * u, 2), source_chips(pick_of(SEND, step))]
        await_slabs(disp_rs.at[step], step == SEND.index(0))
        to_tp(block, block, row_ss, row_rs.at[step], mate).start()

    def stage_gate_up(chips, which, sem):
        gate = up = None
        for k in range(X):
            x = rows[k, chips].reshape(Y * CAP, 512)
            g = jnp.dot(x, wg[which, k * 512 : (k + 1) * 512, :], preferred_element_type=jnp.float32)
            v = jnp.dot(x, wu[which, k * 512 : (k + 1) * 512, :], preferred_element_type=jnp.float32)
            gate, up = (g, v) if k == 0 else (gate + g, up + v)
        h = gate / (1.0 + jnp.exp(-gate)) * up
        place = (tp, pair)[which]
        hid[place, chips] = h.reshape(Y, CAP, 256).astype(jnp.bfloat16)
        to_tp(hid.at[place, chips], hid.at[place, chips], hid_ss, sem, mate).start()

    def stage_down(step, which):
        offset = pick_of((SEND, BACK)[which], step)
        chips = source_chips(offset)
        out = None
        for k in range(X):
            h = hid[k, chips].reshape(Y * CAP, 256)
            o = jnp.dot(h, wd[which, k * 256 : (k + 1) * 256, :], preferred_element_type=jnp.float32)
            out = o if k == 0 else out + o
        res[which, chips] = out.reshape(Y, CAP, 512).astype(jnp.bfloat16)

        @pl.loop(0, Y)
        def _(j):
            goal = lax.rem(z + Z - offset, Z) * Y + j
            target = goal * C + which

            @pl.when(target != ep)
            def _():
                to_ep(res.at[which, goal], ret.at[ep], ret_ss.at[which], ret_rs.at[step], target).start()

            @pl.when(target == ep)
            def _():
                ret[ep] = res[which, goal]

    def stage_combine(step):
        offset = jnp.where(core == 0, pick_of(SEND, step), pick_of(BACK, step))
        plane = lax.rem(z + offset, Z)
        await_slabs(ret_rs.at[step], offset == 0)
        index = lax.broadcasted_iota(jnp.int32, (count, PLANE * CAP), 1) + plane * (PLANE * CAP)
        index = index.astype(jnp.float32)
        share = jnp.where(cols[0][:, 0:1] == index, cols[2][:, 0:1], 0.0)
        share = jnp.where(cols[1][:, 0:1] == index, cols[3][:, 0:1], share)
        high = share.astype(jnp.bfloat16)
        low = (share - high.astype(jnp.float32)).astype(jnp.bfloat16)
        got = ret[pl.ds(plane * PLANE, PLANE)].reshape(PLANE * CAP, 512)
        acc[...] += jnp.dot(high, got, preferred_element_type=jnp.float32) + jnp.dot(
            low, got, preferred_element_type=jnp.float32
        )

    acc[...] = jnp.zeros(acc.shape, jnp.float32)

    def stage_own(step):
        chips = source_chips(pick_of(SEND, step))
        await_recv(rows.at[pl.ds(2 * (1 - u), 2), chips], row_rs.at[step])
        stage_gate_up(chips, 0, hid_rs.at[0, step])

    def stage_pair(step):
        stage_gate_up(source_chips(pick_of(SEND, step)), 1, hid_rs.at[1, step])

    def stage_down_own(step):
        chips = source_chips(pick_of(SEND, step))
        await_recv(hid.at[mate, chips], hid_rs.at[0, step])
        await_recv(hid.at[far, chips], hid_rs.at[1, step])
        stage_down(step, 0)

    @pl.loop(0, DOWN + Z // 2)
    def _(s):
        @pl.when(s < Z)
        def _():
            stage_rows(s)

        @pl.when((s >= 1) & (s < Z + 1))
        def _():
            stage_own(s - 1)

        @pl.when(s == PAIR)
        def _():
            await_recv(wg.at[1], wt_rs.at[0])
            await_recv(wu.at[1], wt_rs.at[1])

        @pl.when((s >= PAIR) & (s < PAIR + Z // 2))
        def _():
            stage_pair(2 * (s - PAIR))
            stage_pair(2 * (s - PAIR) + 1)

        @pl.when(s == PAIR + Z // 2)
        def _():
            await_recv(mrows.at[pair], mix_rs.at[0])
            to_tp(mrows.at[pair], mrows.at[pair], mix_ss.at[2], mix_rs.at[2], mate).start()

        @pl.when(s >= DOWN)
        def _():
            stage_down_own(2 * (s - DOWN))
            stage_down_own(2 * (s - DOWN) + 1)

    await_recv(mrows.at[mate], mix_rs.at[1])
    for load in loads[3:]:
        load.wait()
    await_recv(mrows.at[far], mix_rs.at[2])

    @pl.loop(0, 2)
    def _(n):
        span = pl.ds(pl.multiple_of(n * 256, 256), 256)
        m = mrows[...].reshape(count, 2048)
        in_gate = jnp.dot(m, wi[:, span], preferred_element_type=jnp.float32)
        values = jnp.dot(m, wv[:, span], preferred_element_type=jnp.float32)
        product = (in_gate * values).astype(jnp.bfloat16)
        ext[8:, span] = product.astype(jnp.float32)
        rim_s[:, span] = product[count - 16 :]
        ogate[:, span] = jnp.dot(m, wo[:, span], preferred_element_type=jnp.float32)

    to_ep(rim_s, rim_r, rim_ss, rim_rs, lax.rem(ep + 1, EP)).start()

    await_recv(wd.at[1], wt_rs.at[2])

    @pl.loop(0, Z)
    def _(s):
        stage_down(s, 1)

    await_recv(rim_r, rim_rs)
    before = rim_r[...].astype(jnp.float32)[8:]
    ext[0:8, :] = jnp.where(ep == 0, jnp.zeros_like(before), before)

    @pl.loop(0, 4)
    def _(n):
        span = pl.ds(pl.multiple_of(n * 128, 128), 128)
        tap_span = pl.ds(pl.multiple_of(tp * 512 + n * 128, 128), 128)
        conv = taps[0:1, tap_span] * ext[6 : 6 + count, span]
        conv = conv + taps[1:2, tap_span] * ext[7 : 7 + count, span]
        conv = conv + taps[2:3, tap_span] * ext[8 : 8 + count, span]
        gat[tp, :, span] = (ogate[:, span] * conv).astype(jnp.bfloat16)

    to_tp(gat.at[tp], gat.at[tp], gat_ss.at[0], gat_rs.at[0], pair).start()
    to_tp(gat.at[tp], gat.at[tp], gat_ss.at[1], gat_rs.at[1], mate).start()

    @pl.loop(0, Z - 3)
    def _(s):
        stage_combine(s)

    await_recv(gat.at[pair], gat_rs.at[0])
    to_tp(gat.at[pair], gat.at[pair], gat_ss.at[2], gat_rs.at[2], mate).start()

    @pl.loop(Z - 3, Z)
    def _(s):
        stage_combine(s)

    fin[...] = acc[...].astype(jnp.bfloat16).reshape(C, count // 2, 512)

    @pl.when(core == 0)
    def _():
        to_ep(fin.at[1], fin_same, fin_ss.at[0], fin_rs.at[0], twin).start()

    @pl.when(core == 1)
    def _():
        to_tp(fin.at[1], fin_pair, fin_ss.at[0], fin_rs.at[1], pair).start()
        to_twin(fin.at[0], fin_pair, fin_ss.at[1], fin_rs.at[1], pair).start()

    await_recv(gat.at[mate], gat_rs.at[1])
    await_recv(gat.at[far], gat_rs.at[2])

    @pl.loop(0, 2)
    def _(n):
        span = pl.ds(pl.multiple_of(n * 256, 256), 256)
        out = None
        for k in range(X):
            o = jnp.dot(gat[k], wp[k * 512 : (k + 1) * 512, span], preferred_element_type=jnp.float32)
            out = o if k == 0 else out + o
        mixer_out[:, span] = out.astype(jnp.bfloat16)

    own = count // 4

    @pl.when(core == 0)
    def _():
        expert_out[first] = fin[0, 0:own]
        expert_out[lax.rem(first + 1, X)] = fin[0, own:]
        await_send(fin.at[1], fin_ss.at[0])

    @pl.when(core == 1)
    def _():
        await_recv(fin_same, fin_rs.at[0])
        expert_out[first] = fin_same[0:own]
        expert_out[lax.rem(first + 1, X)] = fin_same[own:]
        await_send(fin.at[1], fin_ss.at[0])
        await_send(fin.at[0], fin_ss.at[1])

    await_recv(fin_pair, fin_rs.at[1])
    expert_out[lax.rem(first + 2, X)] = fin_pair[0:own]
    expert_out[lax.rem(first + 3, X)] = fin_pair[own:]

    await_send(route.at[0], route_ss)
    await_send(send.at[pl.ds(0, 12)], tok_ss)
    await_send(rim_s, rim_ss)
    for buf, sem in ((wg.at[0], wt_ss.at[0]), (wu.at[0], wt_ss.at[1]), (wd.at[0], wt_ss.at[2])):
        await_send(buf, sem)
    for i in range(3):
        await_send(mrows.at[0], mix_ss.at[i])
        await_send(gat.at[0], gat_ss.at[i])
    await_send(send.at[pl.ds(0, EP - 1)], disp_ss)
    await_send(rows.at[pl.ds(0, 2)], row_ss)
    await_send(hid.at[pl.ds(0, 2)], hid_ss)
    for which in range(C):

        @pl.when(core == which)
        def _():
            await_send(ret.at[pl.ds(0, CHIPS - 1)], ret_ss.at[which])

        @pl.when(core != which)
        def _():
            await_send(ret.at[pl.ds(0, CHIPS)], ret_ss.at[which])


def hand_over(mixer_in, expert_in, mixer_out, expert_out, held, in_sem, out_sem):
    ins = [pltpu.make_async_copy(src, held.at[i], in_sem.at[i]) for i, src in enumerate((mixer_in, expert_in))]
    outs = [pltpu.make_async_copy(held.at[i], dst, out_sem.at[i]) for i, dst in enumerate((mixer_out, expert_out))]
    for copy in ins:
        copy.start()
    for i in range(2):
        ins[i].wait()
        outs[i].start()
    for copy in outs:
        copy.wait()


def on_device(
    mixer_in, expert_in, mixer_gain, in_gate_weight, out_gate_weight, value_weight, conv_taps, mixer_proj,
    expert_gain, route_ids, route_weights, gate_weight, up_weight, down_weight,
):
    bf16, f32 = jnp.bfloat16, jnp.float32
    own, wide = mixer_in.shape
    count = route_ids.shape[0]
    local = pl.BlockSpec(memory_space=pltpu.VMEM)
    remote = pl.BlockSpec(memory_space=pl.ANY)
    dma, vmem = pltpu.SemaphoreType.DMA, pltpu.VMEM
    out = jax.ShapeDtypeStruct((count, 512), bf16)
    results = pl.pallas_call(
        kernel,
        out_shape=(out, jax.ShapeDtypeStruct((X, own, 512), bf16)),
        in_specs=[local] * 7 + [remote] * 7,
        out_specs=(local, local),
        scratch_shapes=[
            *[vmem((wide, 512), bf16)] * 4, *[vmem((2, wide, 256), bf16)] * 2, vmem((2, 1024, 512), bf16),
            vmem((C, 8, count), f32), vmem((X, own, 512), bf16), vmem((C, 2, own, 512), bf16), vmem((X, own, wide), bf16),
            vmem((EP, CAP, 512), bf16), vmem((X, CHIPS, CAP, 512), bf16), vmem((X, CHIPS, CAP, 256), bf16),
            vmem((C, CHIPS, CAP, 512), bf16), vmem((EP, CAP, 512), bf16), vmem((X, count, 512), bf16),
            vmem((count + 8, 512), f32), vmem((count, 512), f32), vmem((count, 512), f32),
            vmem((16, 512), bf16), vmem((16, 512), bf16), vmem((8, count), f32), vmem((4, count, 128), f32),
            vmem((C, count // 2, 512), bf16), vmem((count // 2, 512), bf16), vmem((count // 2, 512), bf16),
            dma((7,)), dma((3,)), dma((3,)), dma, dma, dma, dma, dma((3,)), dma((3,)), dma, dma((Z,)), dma, dma((Z,)),
            dma, dma((2, Z)), dma((2,)), dma((Z,)), dma((3,)), dma((3,)), dma, dma, dma((2,)), dma((2,)),
        ],
        compiler_params=pltpu.CompilerParams(
            collective_id=0, has_side_effects=True, vmem_limit_bytes=62 * 2**20
        ),
        name="mixer_and_experts",
    )(
        mixer_in, expert_in, mixer_gain.reshape(1, -1), expert_gain.reshape(1, -1), conv_taps,
        route_ids.T, route_weights.T,
        in_gate_weight, out_gate_weight, value_weight, mixer_proj, gate_weight[0], up_weight[0], down_weight[0],
    )
    return pl.pallas_call(
        hand_over,
        out_shape=(out, out),
        in_specs=[remote] * 2,
        out_specs=(remote, remote),
        scratch_shapes=[vmem((2, count, 512), bf16), dma((2,)), dma((2,))],
        name="hand_over",
    )(results[0], results[1].reshape(count, 512))


def solution(mesh):
    return jax.shard_map(
        on_device,
        mesh=mesh,
        in_specs=(
            P(("ep", "tp"), None),
            P(("ep", "tp"), None),
            P(),
            P(None, "tp"),
            P(None, "tp"),
            P(None, "tp"),
            P(),
            P(None, "tp"),
            P(),
            P("ep", None),
            P("ep", None),
            P("ep", None, "tp"),
            P("ep", None, "tp"),
            P("ep", None, "tp"),
        ),
        out_specs=(P("ep", "tp"), P("ep", "tp")),
        check_vma=False,
    )
```

```python
import jax
import jax.numpy as jnp
from jax import lax
from jax.experimental import pallas as pl
from jax.experimental.pallas import tpu as pltpu
from jax.sharding import PartitionSpec as P

norm_eps = 1e-06
Z, Y, C, X = 8, 4, 2, 4
PLANE = Y * C
EP = Z * PLANE
CHIPS = Z * Y
CAP = 24
SEND = (1, 7, 2, 6, 0, 3, 5, 4)
BACK = (4, 3, 5, 2, 6, 1, 7, 0)
EARLY = 4
HALO = 8
MESH = pl.DeviceIdType.MESH


def pick_of(table, step):
    value = table[0]
    for at in range(1, len(table)):
        value = jnp.where(step == at, table[at], value)
    return value


def rms_rows(values, gain_row):
    wide = values.astype(jnp.float32)
    scale = lax.rsqrt(jnp.mean(wide * wide, axis=-1, keepdims=True) + norm_eps)
    return (wide * scale * gain_row).astype(jnp.bfloat16)


def kernel(
    mixer_in, expert_in, mixer_gain, expert_gain, taps, ids, weights,
    wi_hbm, wo_hbm, wv_hbm, wp_hbm, wg_hbm, wu_hbm, wd_hbm,
    mixer_out, expert_out,
    wi, wo, wv, wp, wg, wu, wd,
    route, tok_send, tok, mrows, halo, send, rows, hid, res, res_pair, ret, ret_pair, gat, ext, ogate, acc, slot_rows, cols,
    fin, fin_same, fin_half, fin_pair,
    load_sem, wt_ss, wt_rs, route_ss, route_rs, tok_ss, tok_rs, mix_ss, mix_rs, disp_ss, disp_rs, row_ss, row_rs,
    hid_ss, hid_rs, ret_ss, ret_rs, gat_ss, gat_rs, halo_ss, halo_rs, fin_ss, fin_rs,
):
    ep, tp = lax.axis_index("ep"), lax.axis_index("tp")
    z, core = ep // PLANE, lax.rem(ep, C)
    chip, twin = ep // C, ep + 1 - 2 * core
    odd = lax.rem(tp, 2)
    pair = tp + 1 - 2 * odd
    mate = lax.rem(tp + 3 + 2 * odd, X)
    far = lax.rem(tp + 2, X)
    u = 1 - odd
    first = lax.rem(tp + X - u, X)
    count = ids.shape[1]

    loads = [
        pltpu.make_async_copy(src, dst, load_sem.at[i])
        for i, (src, dst) in enumerate(
            ((wg_hbm, wg.at[0]), (wu_hbm, wu.at[0]), (wd_hbm, wd.at[0]),
             (wi_hbm, wi), (wo_hbm, wo), (wv_hbm, wv), (wp_hbm, wp))
        )
    ]
    for load in loads:
        load.start()

    barrier = pltpu.get_barrier_semaphore()

    @pl.loop(1, EP)
    def _(d):
        pl.semaphore_signal(barrier, inc=1, device_id={"ep": lax.rem(ep + d, EP)}, device_id_type=MESH)

    for other in (pair, mate):
        pl.semaphore_signal(barrier, inc=1, device_id={"tp": other}, device_id_type=MESH)
        pl.semaphore_signal(barrier, inc=1, device_id={"ep": twin, "tp": other}, device_id_type=MESH)

    @pl.when(tp != X - 1)
    def _():
        pl.semaphore_signal(
            barrier, inc=1, device_id={"ep": lax.rem(ep + EP - 1, EP), "tp": X - 1}, device_id_type=MESH
        )

    def to_ep(src, dst, ss, rs, target):
        return pltpu.make_async_remote_copy(src, dst, ss, rs, device_id={"ep": target}, device_id_type=MESH)

    def to_tp(src, dst, ss, rs, target):
        return pltpu.make_async_remote_copy(src, dst, ss, rs, device_id={"tp": target}, device_id_type=MESH)

    def mixer_block(owner):
        return mrows.at[owner]

    def to_twin(src, dst, ss, rs, target):
        return pltpu.make_async_remote_copy(
            src, dst, ss, rs, device_id={"ep": twin, "tp": target}, device_id_type=MESH
        )

    def await_recv(ref, sem):
        to_tp(ref, ref, sem, sem, mate).wait_recv()

    def await_send(ref, sem):
        to_tp(ref, ref, sem, sem, mate).wait_send()

    picks = jnp.concatenate(
        [ids[...].astype(jnp.float32), weights[...], jnp.zeros((4, count), jnp.float32)], axis=0
    )
    turned = jnp.where((first == 1) == (core == 0), pltpu.roll(picks, 3 * count // 4, 1), pltpu.roll(picks, count // 4, 1))
    route[core] = turned
    normed = rms_rows(expert_in[...], expert_gain[...])
    for k in range(X):
        tok_send[k] = normed[:, k * 512 : (k + 1) * 512]
    tok[core, u] = tok_send[2 * u + core]

    for load in loads[:3]:
        load.wait()
    half_a, half_b = pl.ds(0, 256), pl.ds(256, 256)
    pl.semaphore_wait(barrier, EP + 3 + (X - 1) * (tp // (X - 1)))

    to_ep(route.at[core], route.at[core], route_ss, route_rs, twin).start()
    to_twin(tok_send.at[2 * (1 - u) + 1 - core], tok.at[core, u], tok_ss, tok_rs, mate).start()
    to_tp(tok_send.at[2 * (1 - u) + core], tok.at[core, u], tok_ss, tok_rs, mate).start()
    to_ep(tok_send.at[2 * u + 1 - core], tok.at[core, u], tok_ss, tok_rs, twin).start()
    tail_rows = rms_rows(mixer_in[mixer_in.shape[0] - 16 :], mixer_gain[...])
    halo[0] = tail_rows[16 - HALO :]

    @pl.when(tp == X - 1)
    def _():
        for other in range(X):
            pltpu.make_async_remote_copy(
                halo.at[0], halo.at[1], halo_ss, halo_rs,
                device_id={"ep": lax.rem(ep + 1, EP), "tp": other}, device_id_type=MESH,
            ).start()

    to_tp(wg.at[0], wg.at[1], wt_ss.at[0], wt_rs.at[0], pair).start()
    to_tp(wu.at[0], wu.at[1], wt_ss.at[1], wt_rs.at[1], pair).start()
    mrows[tp] = rms_rows(mixer_in[...], mixer_gain[...])
    to_tp(mixer_block(tp), mixer_block(tp), mix_ss.at[0], mix_rs.at[0], pair).start()
    to_tp(wd.at[0, :, half_a], wd.at[1, :, half_a], wt_ss.at[2], wt_rs.at[2], pair).start()
    to_tp(wd.at[0, :, half_b], wd.at[1, :, half_b], wt_ss.at[3], wt_rs.at[3], pair).start()

    await_recv(route.at[1 - core], route_rs)
    lane = lax.broadcasted_iota(jnp.int32, (8, count), 1)
    both = jnp.where(lane < count // 2, route[0], route[1])
    labels = lax.broadcasted_iota(jnp.int32, (EP, count), 0).astype(jnp.float32)
    hot = [both[k : k + 1, :] == labels for k in range(2)]
    named = jnp.where(hot[0] | hot[1], 1.0, 0.0).astype(jnp.bfloat16)
    older = (
        lax.broadcasted_iota(jnp.int32, (count, count), 0) < lax.broadcasted_iota(jnp.int32, (count, count), 1)
    )
    earlier = jnp.dot(named, jnp.where(older, 1.0, 0.0).astype(jnp.bfloat16), preferred_element_type=jnp.float32)
    for k in range(2):
        within = jnp.sum(jnp.where(hot[k], earlier, 0.0), axis=0, keepdims=True)
        slot = both[k : k + 1, :] * CAP + within
        slot_rows[k : k + 1, :] = slot

    await_recv(send.at[pl.ds(0, 12)], tok_rs)
    to_tp(mixer_block(tp), mixer_block(tp), mix_ss.at[1], mix_rs.at[1], mate).start()

    @pl.loop(0, Z)
    def _(step):
        plane = lax.rem(z + pick_of(SEND, step), Z)
        index = (lax.broadcasted_iota(jnp.int32, (PLANE * CAP, count), 0) + plane * (PLANE * CAP)).astype(jnp.float32)
        pick = (index == slot_rows[0:1, :]) | (index == slot_rows[1:2, :])
        moved = jnp.dot(
            jnp.where(pick, 1.0, 0.0).astype(jnp.bfloat16),
            tok[...].reshape(count, 512),
            preferred_element_type=jnp.float32,
        )
        send[pl.ds(plane * PLANE, PLANE)] = moved.reshape(PLANE, CAP, 512).astype(jnp.bfloat16)

        @pl.loop(0, PLANE)
        def _(j):
            target = plane * PLANE + j

            @pl.when(target != ep)
            def _():
                to_ep(send.at[target], rows.at[2 * u + core, chip], disp_ss, disp_rs.at[step], target).start()

            @pl.when(target == ep)
            def _():
                rows[2 * u + core, chip] = send[ep]

    total = both[2:3, :] + both[3:4, :]
    for k in range(2):
        cols[k] = jnp.transpose(jnp.broadcast_to(slot_rows[k : k + 1, :], (128, count)))
        cols[2 + k] = jnp.transpose(jnp.broadcast_to(both[2 + k : 3 + k, :] / total, (128, count)))

    def source_chips(offset):
        return pl.ds(lax.rem(z + Z - offset, Z) * Y, Y)

    def await_slabs(sem, last):
        @pl.when(last)
        def _():
            await_recv(send.at[pl.ds(0, PLANE - 1)], sem)

        @pl.when(jnp.logical_not(last))
        def _():
            await_recv(send.at[pl.ds(0, PLANE)], sem)

    def stage_rows(step):
        block = rows.at[pl.ds(2 * u, 2), source_chips(pick_of(SEND, step))]
        await_slabs(disp_rs.at[step], step == SEND.index(0))
        to_tp(block, block, row_ss, row_rs.at[step], mate).start()

    def stage_gate_up(chips, which, sem):
        gate = up = None
        for k in range(X):
            x = rows[k, chips].reshape(Y * CAP, 512)
            g = jnp.dot(x, wg[which, k * 512 : (k + 1) * 512, :], preferred_element_type=jnp.float32)
            v = jnp.dot(x, wu[which, k * 512 : (k + 1) * 512, :], preferred_element_type=jnp.float32)
            gate, up = (g, v) if k == 0 else (gate + g, up + v)
        h = gate / (1.0 + jnp.exp(-gate)) * up
        place = (tp, pair)[which]
        hid[place, chips] = h.reshape(Y, CAP, 256).astype(jnp.bfloat16)
        to_tp(hid.at[place, chips], hid.at[place, chips], hid_ss, sem, mate).start()

    def down(chips, weight):
        out = None
        for k in range(X):
            h = hid[k, chips].reshape(Y * CAP, 256)
            o = jnp.dot(h, weight(k), preferred_element_type=jnp.float32)
            out = o if k == 0 else out + o
        return out.astype(jnp.bfloat16)

    def stage_down(step):
        offset = pick_of(SEND, step)
        chips = source_chips(offset)
        res[chips] = down(chips, lambda k: wd[0, k * 256 : (k + 1) * 256, :]).reshape(Y, CAP, 512)

        @pl.loop(0, Y)
        def _(j):
            goal = lax.rem(z + Z - offset, Z) * Y + j

            @pl.when(goal * C != ep)
            def _():
                to_ep(res.at[goal], ret.at[ep], ret_ss.at[0], ret_rs.at[0, step], goal * C).start()

            @pl.when(goal * C == ep)
            def _():
                ret[ep] = res[goal]

    def stage_down_pair(step, part):
        offset = pick_of(BACK, step)
        chips = source_chips(offset)
        span = slice(part * 256, (part + 1) * 256)
        res_pair[part, chips] = down(chips, lambda k: wd[1, k * 256 : (k + 1) * 256, span]).reshape(Y, CAP, 256)

        @pl.loop(0, Y)
        def _(j):
            goal = lax.rem(z + Z - offset, Z) * Y + j
            src, dst = res_pair.at[part, goal], ret_pair.at[part, ep]

            @pl.when(goal * C + 1 != ep)
            def _():
                to_ep(src, dst, ret_ss.at[1 + part], ret_rs.at[1 + part, step], goal * C + 1).start()

            @pl.when(goal * C + 1 == ep)
            def _():
                ret_pair[part, ep] = res_pair[part, goal]

    def shares_of(plane):
        index = lax.broadcasted_iota(jnp.int32, (count, PLANE * CAP), 1) + plane * (PLANE * CAP)
        index = index.astype(jnp.float32)
        share = jnp.where(cols[0][:, 0:1] == index, cols[2][:, 0:1], 0.0)
        share = jnp.where(cols[1][:, 0:1] == index, cols[3][:, 0:1], share)
        high = share.astype(jnp.bfloat16)
        return high, (share - high.astype(jnp.float32)).astype(jnp.bfloat16)

    def stage_combine(step):
        offset = pick_of(SEND, step)
        plane = lax.rem(z + offset, Z)
        await_slabs(ret_rs.at[0, step], offset == 0)
        got = ret[pl.ds(plane * PLANE, PLANE)].reshape(PLANE * CAP, 512)
        high, low = shares_of(plane)
        acc[...] += jnp.dot(high, got, preferred_element_type=jnp.float32) + jnp.dot(
            low, got, preferred_element_type=jnp.float32
        )

    def stage_combine_pair(step, part):
        offset = pick_of(BACK, step)
        plane = lax.rem(z + offset, Z)

        @pl.when(offset == 0)
        def _():
            await_recv(ret_pair.at[part, pl.ds(0, PLANE - 1)], ret_rs.at[1 + part, step])

        @pl.when(offset != 0)
        def _():
            await_recv(ret_pair.at[part, pl.ds(0, PLANE)], ret_rs.at[1 + part, step])

        got = ret_pair[part, pl.ds(plane * PLANE, PLANE)].reshape(PLANE * CAP, 256)
        high, low = shares_of(plane)
        acc[:, part * 256 : (part + 1) * 256] += jnp.dot(high, got, preferred_element_type=jnp.float32) + jnp.dot(
            low, got, preferred_element_type=jnp.float32
        )

    acc[...] = jnp.zeros(acc.shape, jnp.float32)

    def stage_own(step):
        chips = source_chips(pick_of(SEND, step))
        await_recv(rows.at[pl.ds(2 * (1 - u), 2), chips], row_rs.at[step])
        stage_gate_up(chips, 0, hid_rs.at[0, step])

    def stage_pair(step):
        stage_gate_up(source_chips(pick_of(SEND, step)), 1, hid_rs.at[1, step])

    def stage_down_own(step):
        chips = source_chips(pick_of(SEND, step))
        await_recv(hid.at[mate, chips], hid_rs.at[0, step])
        await_recv(hid.at[far, chips], hid_rs.at[1, step])
        stage_down(step)

    @pl.loop(0, Z - 1)
    def _(s):
        stage_rows(s)

        @pl.when(s >= 1)
        def _():
            stage_own(s - 1)

    await_recv(wg.at[1], wt_rs.at[0])
    await_recv(wu.at[1], wt_rs.at[1])

    @pl.loop(0, EARLY)
    def _(s):
        stage_pair(s)

    stage_rows(Z - 1)
    stage_own(Z - 2)

    @pl.loop(EARLY, Z - 1)
    def _(s):
        stage_pair(s)

    @pl.loop(0, EARLY)
    def _(s):
        stage_down_own(s)

    stage_own(Z - 1)
    stage_pair(Z - 1)
    await_recv(mixer_block(pair), mix_rs.at[0])
    to_tp(mixer_block(pair), mixer_block(pair), mix_ss.at[2], mix_rs.at[2], mate).start()

    @pl.loop(EARLY, Z)
    def _(s):
        stage_down_own(s)

    await_recv(wd.at[1, :, half_a], wt_rs.at[2])

    @pl.loop(0, Z)
    def _(s):
        stage_down_pair(s, 0)

    await_recv(halo.at[1], halo_rs)
    await_recv(mixer_block(mate), mix_rs.at[1])
    for load in loads[3:]:
        load.wait()
    await_recv(mixer_block(far), mix_rs.at[2])

    for n in range(2):
        span = slice(n * 256, (n + 1) * 256)
        m, before = mrows[...].reshape(count, 2048), halo[1]
        in_gate = jnp.dot(m, wi[:, span], preferred_element_type=jnp.float32)
        values = jnp.dot(m, wv[:, span], preferred_element_type=jnp.float32)
        ext[HALO:, :] = (in_gate * values).astype(jnp.bfloat16).astype(jnp.float32)
        in_gate = jnp.dot(before, wi[:, span], preferred_element_type=jnp.float32)
        values = jnp.dot(before, wv[:, span], preferred_element_type=jnp.float32)
        product = (in_gate * values).astype(jnp.bfloat16).astype(jnp.float32)
        ext[0:HALO, :] = jnp.where(ep == 0, 0.0, product)
        ogate[...] = jnp.dot(m, wo[:, span], preferred_element_type=jnp.float32)

        for i in range(2):
            lanes = slice(i * 128, (i + 1) * 128)
            tap_span = pl.ds(pl.multiple_of(tp * 512 + n * 256 + i * 128, 128), 128)
            conv = taps[0:1, tap_span] * ext[HALO - 2 : HALO - 2 + count, lanes]
            conv = conv + taps[1:2, tap_span] * ext[HALO - 1 : HALO - 1 + count, lanes]
            conv = conv + taps[2:3, tap_span] * ext[HALO:, lanes]
            gat[tp, n, :, lanes] = (ogate[:, lanes] * conv).astype(jnp.bfloat16)

        to_tp(gat.at[tp, n], gat.at[tp, n], gat_ss.at[0], gat_rs.at[0, n], pair).start()
        to_tp(gat.at[tp, n], gat.at[tp, n], gat_ss.at[1], gat_rs.at[1, n], mate).start()

    await_recv(wd.at[1, :, half_b], wt_rs.at[3])

    @pl.loop(0, Z)
    def _(s):
        stage_down_pair(s, 1)

    for n in range(2):
        await_recv(gat.at[pair, n], gat_rs.at[0, n])
        to_tp(gat.at[pair, n], gat.at[pair, n], gat_ss.at[2], gat_rs.at[2, n], mate).start()

    @pl.when(core == 0)
    def _():
        @pl.loop(0, Z)
        def _(s):
            stage_combine(s)

        fin[...] = acc[...].astype(jnp.bfloat16).reshape(C, count // 2, 512)
        to_ep(fin.at[1], fin_same, fin_ss.at[0], fin_rs.at[0], twin).start()

    def finish_pair(part):
        @pl.when(core == 1)
        def _():
            @pl.loop(0, Z)
            def _(s):
                stage_combine_pair(s, part)

            fin_half[part] = acc[:, part * 256 : (part + 1) * 256].astype(jnp.bfloat16).reshape(C, count // 2, 256)
            to_tp(fin_half.at[part, 1], fin_pair.at[part], fin_ss.at[0], fin_rs.at[1 + part], pair).start()
            to_twin(fin_half.at[part, 0], fin_pair.at[part], fin_ss.at[1], fin_rs.at[1 + part], pair).start()

    finish_pair(0)
    finish_pair(1)
    for n in range(2):
        await_recv(gat.at[mate, n], gat_rs.at[1, n])
        await_recv(gat.at[far, n], gat_rs.at[2, n])

    @pl.loop(0, 2)
    def _(n):
        span = pl.ds(pl.multiple_of(n * 256, 256), 256)
        out = None
        for k in range(2 * X):
            part = gat[k // 2, k % 2]
            o = jnp.dot(part, wp[k * 256 : (k + 1) * 256, span], preferred_element_type=jnp.float32)
            out = o if k == 0 else out + o
        mixer_out[:, span] = out.astype(jnp.bfloat16)

    own = count // 4

    @pl.when(core == 0)
    def _():
        expert_out[first] = fin[0, 0:own]
        expert_out[lax.rem(first + 1, X)] = fin[0, own:]
        await_send(fin.at[1], fin_ss.at[0])

    @pl.when(core == 1)
    def _():
        await_recv(fin_same, fin_rs.at[0])
        expert_out[first] = fin_same[0:own]
        expert_out[lax.rem(first + 1, X)] = fin_same[own:]
        await_send(fin_half.at[0], fin_ss.at[0])
        await_send(fin_half.at[0], fin_ss.at[1])

    for part in range(2):
        await_recv(fin_pair.at[part], fin_rs.at[1 + part])
        expert_out[lax.rem(first + 2, X), :, part * 256 : (part + 1) * 256] = fin_pair[part, 0:own]
        expert_out[lax.rem(first + 3, X), :, part * 256 : (part + 1) * 256] = fin_pair[part, own:]

    await_send(route.at[0], route_ss)
    await_send(send.at[pl.ds(0, 12)], tok_ss)
    await_send(wg.at[0], wt_ss.at[0])
    await_send(wu.at[0], wt_ss.at[1])
    await_send(wd.at[0, :, half_a], wt_ss.at[2])
    await_send(wd.at[0, :, half_b], wt_ss.at[3])
    for i in range(3):
        await_send(mixer_block(0), mix_ss.at[i])
        await_send(gat.at[0], gat_ss.at[i])
    await_send(send.at[pl.ds(0, EP - 1)], disp_ss)
    await_send(rows.at[pl.ds(0, 2)], row_ss)
    await_send(hid.at[pl.ds(0, 2)], hid_ss)

    @pl.when(tp == X - 1)
    def _():
        for _ in range(X):
            await_send(halo.at[0], halo_ss)

    @pl.when(core == 0)
    def _():
        await_send(ret.at[pl.ds(0, CHIPS - 1)], ret_ss.at[0])
        await_send(ret_pair.at[0, pl.ds(0, CHIPS)], ret_ss.at[1])
        await_send(ret_pair.at[0, pl.ds(0, CHIPS)], ret_ss.at[2])

    @pl.when(core == 1)
    def _():
        await_send(ret.at[pl.ds(0, CHIPS)], ret_ss.at[0])
        await_send(ret_pair.at[0, pl.ds(0, CHIPS - 1)], ret_ss.at[1])
        await_send(ret_pair.at[0, pl.ds(0, CHIPS - 1)], ret_ss.at[2])


def hand_over(mixer_in, expert_in, mixer_out, expert_out, held, in_sem, out_sem):
    ins = [pltpu.make_async_copy(src, held.at[i], in_sem.at[i]) for i, src in enumerate((mixer_in, expert_in))]
    outs = [pltpu.make_async_copy(held.at[i], dst, out_sem.at[i]) for i, dst in enumerate((mixer_out, expert_out))]
    for copy in ins:
        copy.start()
    for i in range(2):
        ins[i].wait()
        outs[i].start()
    for copy in outs:
        copy.wait()


def on_device(
    mixer_in, expert_in, mixer_gain, in_gate_weight, out_gate_weight, value_weight, conv_taps, mixer_proj,
    expert_gain, route_ids, route_weights, gate_weight, up_weight, down_weight,
):
    bf16, f32 = jnp.bfloat16, jnp.float32
    own, wide = mixer_in.shape
    count = route_ids.shape[0]
    local = pl.BlockSpec(memory_space=pltpu.VMEM)
    remote = pl.BlockSpec(memory_space=pl.ANY)
    dma, vmem = pltpu.SemaphoreType.DMA, pltpu.VMEM
    out = jax.ShapeDtypeStruct((count, 512), bf16)
    results = pl.pallas_call(
        kernel,
        out_shape=(out, jax.ShapeDtypeStruct((X, own, 512), bf16)),
        in_specs=[local] * 7 + [remote] * 7,
        out_specs=(local, local),
        scratch_shapes=[
            *[vmem((wide, 512), bf16)] * 4, *[vmem((2, wide, 256), bf16)] * 2, vmem((2, 1024, 512), bf16),
            vmem((C, 8, count), f32), vmem((X, own, 512), bf16), vmem((C, 2, own, 512), bf16),
            vmem((X, own, wide), bf16), vmem((2, HALO, wide), bf16),
            vmem((EP, CAP, 512), bf16), vmem((X, CHIPS, CAP, 512), bf16), vmem((X, CHIPS, CAP, 256), bf16),
            vmem((CHIPS, CAP, 512), bf16), vmem((2, CHIPS, CAP, 256), bf16),
            vmem((EP, CAP, 512), bf16), vmem((2, EP, CAP, 256), bf16), vmem((X, 2, count, 256), bf16),
            vmem((HALO + count, 256), f32), vmem((count, 256), f32), vmem((count, 512), f32),
            vmem((8, count), f32), vmem((4, count, 128), f32),
            vmem((C, count // 2, 512), bf16), vmem((count // 2, 512), bf16),
            vmem((2, C, count // 2, 256), bf16), vmem((2, count // 2, 256), bf16),
            dma((7,)), dma((4,)), dma((4,)), dma, dma, dma, dma, dma((3,)), dma((3,)), dma, dma((Z,)), dma, dma((Z,)),
            dma, dma((2, Z)), dma((3,)), dma((3, Z)), dma((3,)), dma((3, 2)), dma, dma, dma((2,)), dma((3,)),
        ],
        compiler_params=pltpu.CompilerParams(
            collective_id=0, has_side_effects=True, vmem_limit_bytes=62 * 2**20
        ),
        name="mixer_and_experts",
    )(
        mixer_in, expert_in, mixer_gain.reshape(1, -1), expert_gain.reshape(1, -1), conv_taps,
        route_ids.T, route_weights.T,
        in_gate_weight, out_gate_weight, value_weight, mixer_proj, gate_weight[0], up_weight[0], down_weight[0],
    )
    return pl.pallas_call(
        hand_over,
        out_shape=(out, out),
        in_specs=[remote] * 2,
        out_specs=(remote, remote),
        scratch_shapes=[vmem((2, count, 512), bf16), dma((2,)), dma((2,))],
        name="hand_over",
    )(results[0], results[1].reshape(count, 512))


def solution(mesh):
    return jax.shard_map(
        on_device,
        mesh=mesh,
        in_specs=(
            P(("ep", "tp"), None),
            P(("ep", "tp"), None),
            P(),
            P(None, "tp"),
            P(None, "tp"),
            P(None, "tp"),
            P(),
            P(None, "tp"),
            P(),
            P("ep", None),
            P("ep", None),
            P("ep", None, "tp"),
            P("ep", None, "tp"),
            P("ep", None, "tp"),
        ),
        out_specs=(P("ep", "tp"), P("ep", "tp")),
        check_vma=False,
    )
```

```python
import jax
import jax.numpy as jnp
from jax import lax
from jax.experimental import pallas as pl
from jax.experimental.pallas import tpu as pltpu
from jax.sharding import PartitionSpec as P

norm_eps = 1e-06
Z, Y, C, X = 8, 4, 2, 4
PLANE = Y * C
EP = Z * PLANE
CHIPS = Z * Y
CAP = 24
SEND = (1, 7, 2, 6, 0, 3, 5, 4)
BACK = (4, 3, 5, 2, 6, 1, 7, 0)
SPANS = (slice(0, 256), slice(256, 512))
EARLY = 4
HALO = 8
MESH = pl.DeviceIdType.MESH


def pick_of(table, step):
    value = table[0]
    for at in range(1, len(table)):
        value = jnp.where(step == at, table[at], value)
    return value


def rms_rows(values, gain_row):
    wide = values.astype(jnp.float32)
    scale = lax.rsqrt(jnp.mean(wide * wide, axis=-1, keepdims=True) + norm_eps)
    return (wide * scale * gain_row).astype(jnp.bfloat16)


def kernel(
    mixer_in, expert_in, mixer_gain, expert_gain, taps, ids, weights,
    wi_hbm, wo_hbm, wv_hbm, wp_hbm, wg_hbm, wu_hbm, wd_hbm,
    mixer_out, expert_out,
    wi, wo, wv, wp, wg, wu, wd,
    route, tok_send, tok, mrows, halo, send, rows, hid, res, res_pair_a, res_pair_b, ret, ret_pair_a, ret_pair_b, gat, ext, ogate, acc, slot_rows, cols,
    fin, fin_same, fin_half_a, fin_half_b, fin_pair_a, fin_pair_b, picks_of, shares, mixed,
    load_sem, store_sem, wt_ss, wt_rs, route_ss, route_rs, tok_ss, tok_rs, mix_ss, mix_rs, disp_ss, disp_rs, row_ss, row_rs,
    hid_ss, hid_rs, ret_ss, ret_rs, gat_ss, gat_rs, halo_ss, halo_rs, fin_ss, fin_rs,
):
    ep, tp = lax.axis_index("ep"), lax.axis_index("tp")
    res_pair, ret_pair = (res_pair_a, res_pair_b), (ret_pair_a, ret_pair_b)
    fin_half, fin_pair = (fin_half_a, fin_half_b), (fin_pair_a, fin_pair_b)
    z, core = ep // PLANE, lax.rem(ep, C)
    chip, twin = ep // C, ep + 1 - 2 * core
    odd = lax.rem(tp, 2)
    pair = tp + 1 - 2 * odd
    mate = lax.rem(tp + 3 + 2 * odd, X)
    far = lax.rem(tp + 2, X)
    u = 1 - odd
    first = lax.rem(tp + X - u, X)
    count = ids.shape[1]

    loads = [
        pltpu.make_async_copy(src, dst, load_sem.at[i])
        for i, (src, dst) in enumerate(
            ((wg_hbm, wg.at[0]), (wu_hbm, wu.at[0]), (wd_hbm, wd.at[0]),
             (wi_hbm, wi), (wo_hbm, wo), (wv_hbm, wv), (wp_hbm, wp))
        )
    ]
    for load in loads:
        load.start()

    barrier = pltpu.get_barrier_semaphore()

    @pl.loop(1, EP)
    def _(d):
        pl.semaphore_signal(barrier, inc=1, device_id={"ep": lax.rem(ep + d, EP)}, device_id_type=MESH)

    for other in (pair, mate):
        pl.semaphore_signal(barrier, inc=1, device_id={"tp": other}, device_id_type=MESH)
        pl.semaphore_signal(barrier, inc=1, device_id={"ep": twin, "tp": other}, device_id_type=MESH)

    @pl.when(tp != X - 1)
    def _():
        pl.semaphore_signal(
            barrier, inc=1, device_id={"ep": lax.rem(ep + EP - 1, EP), "tp": X - 1}, device_id_type=MESH
        )

    def to_ep(src, dst, ss, rs, target):
        return pltpu.make_async_remote_copy(src, dst, ss, rs, device_id={"ep": target}, device_id_type=MESH)

    def to_tp(src, dst, ss, rs, target):
        return pltpu.make_async_remote_copy(src, dst, ss, rs, device_id={"tp": target}, device_id_type=MESH)

    def mixer_block(owner):
        return mrows.at[owner]

    def to_twin(src, dst, ss, rs, target):
        return pltpu.make_async_remote_copy(
            src, dst, ss, rs, device_id={"ep": twin, "tp": target}, device_id_type=MESH
        )

    def await_recv(ref, sem):
        to_tp(ref, ref, sem, sem, mate).wait_recv()

    def await_send(ref, sem):
        to_tp(ref, ref, sem, sem, mate).wait_send()

    picks = jnp.concatenate(
        [ids[...].astype(jnp.float32), weights[...], jnp.zeros((4, count), jnp.float32)], axis=0
    )
    turned = jnp.where((first == 1) == (core == 0), pltpu.roll(picks, 3 * count // 4, 1), pltpu.roll(picks, count // 4, 1))
    route[core] = turned
    normed = rms_rows(expert_in[...], expert_gain[...])
    for k in range(X):
        tok_send[k] = normed[:, k * 512 : (k + 1) * 512]
    tok[core, u] = tok_send[2 * u + core]

    for load in loads[:3]:
        load.wait()
    half_a, half_b = (pl.ds(span.start, span.stop - span.start) for span in SPANS)
    pl.semaphore_wait(barrier, EP + 3 + (X - 1) * (tp // (X - 1)))

    to_ep(route.at[core], route.at[core], route_ss, route_rs, twin).start()
    to_twin(tok_send.at[2 * (1 - u) + 1 - core], tok.at[core, u], tok_ss, tok_rs, mate).start()
    to_tp(tok_send.at[2 * (1 - u) + core], tok.at[core, u], tok_ss, tok_rs, mate).start()
    to_ep(tok_send.at[2 * u + 1 - core], tok.at[core, u], tok_ss, tok_rs, twin).start()
    tail_rows = rms_rows(mixer_in[mixer_in.shape[0] - 16 :], mixer_gain[...])
    halo[0] = tail_rows[16 - HALO :]

    @pl.when(tp == X - 1)
    def _():
        for other in range(X):
            pltpu.make_async_remote_copy(
                halo.at[0], halo.at[1], halo_ss, halo_rs,
                device_id={"ep": lax.rem(ep + 1, EP), "tp": other}, device_id_type=MESH,
            ).start()

    to_tp(wg.at[0], wg.at[1], wt_ss.at[0], wt_rs.at[0], pair).start()
    to_tp(wu.at[0], wu.at[1], wt_ss.at[1], wt_rs.at[1], pair).start()
    mrows[tp] = rms_rows(mixer_in[...], mixer_gain[...])
    to_tp(mixer_block(tp), mixer_block(tp), mix_ss.at[0], mix_rs.at[0], pair).start()
    to_tp(wd.at[0, :, half_a], wd.at[1, :, half_a], wt_ss.at[2], wt_rs.at[2], pair).start()
    to_tp(wd.at[0, :, half_b], wd.at[1, :, half_b], wt_ss.at[3], wt_rs.at[3], pair).start()

    await_recv(route.at[1 - core], route_rs)
    lane = lax.broadcasted_iota(jnp.int32, (8, count), 1)
    both = jnp.where(lane < count // 2, route[0], route[1])
    labels = lax.broadcasted_iota(jnp.int32, (EP, count), 0).astype(jnp.float32)
    hot = [both[k : k + 1, :] == labels for k in range(2)]
    named = jnp.where(hot[0] | hot[1], 1.0, 0.0).astype(jnp.bfloat16)
    older = (
        lax.broadcasted_iota(jnp.int32, (count, count), 0) < lax.broadcasted_iota(jnp.int32, (count, count), 1)
    )
    earlier = jnp.dot(named, jnp.where(older, 1.0, 0.0).astype(jnp.bfloat16), preferred_element_type=jnp.float32)
    for k in range(2):
        within = jnp.sum(jnp.where(hot[k], earlier, 0.0), axis=0, keepdims=True)
        slot = both[k : k + 1, :] * CAP + within
        slot_rows[k : k + 1, :] = slot

    @pl.loop(0, Z)
    def _(plane):
        index = (lax.broadcasted_iota(jnp.int32, (PLANE * CAP, count), 0) + plane * (PLANE * CAP)).astype(jnp.float32)
        pick = (index == slot_rows[0:1, :]) | (index == slot_rows[1:2, :])
        picks_of[plane] = jnp.where(pick, 1.0, 0.0).astype(jnp.bfloat16)

    await_recv(send.at[pl.ds(0, 12)], tok_rs)
    to_tp(mixer_block(tp), mixer_block(tp), mix_ss.at[1], mix_rs.at[1], mate).start()

    @pl.loop(0, Z)
    def _(step):
        plane = lax.rem(z + pick_of(SEND, step), Z)
        moved = jnp.dot(picks_of[plane], tok[...].reshape(count, 512), preferred_element_type=jnp.float32)
        send[pl.ds(plane * PLANE, PLANE)] = moved.reshape(PLANE, CAP, 512).astype(jnp.bfloat16)

        @pl.loop(0, PLANE)
        def _(j):
            target = plane * PLANE + j

            @pl.when(target != ep)
            def _():
                to_ep(send.at[target], rows.at[2 * u + core, chip], disp_ss, disp_rs.at[step], target).start()

            @pl.when(target == ep)
            def _():
                rows[2 * u + core, chip] = send[ep]

    total = both[2:3, :] + both[3:4, :]
    for k in range(2):
        cols[k] = jnp.transpose(jnp.broadcast_to(slot_rows[k : k + 1, :], (128, count)))
        cols[2 + k] = jnp.transpose(jnp.broadcast_to(both[2 + k : 3 + k, :] / total, (128, count)))

    def source_chips(offset):
        return pl.ds(lax.rem(z + Z - offset, Z) * Y, Y)

    def await_slabs(sem, last):
        @pl.when(last)
        def _():
            await_recv(send.at[pl.ds(0, PLANE - 1)], sem)

        @pl.when(jnp.logical_not(last))
        def _():
            await_recv(send.at[pl.ds(0, PLANE)], sem)

    def stage_rows(step):
        block = rows.at[pl.ds(2 * u, 2), source_chips(pick_of(SEND, step))]
        await_slabs(disp_rs.at[step], step == SEND.index(0))
        to_tp(block, block, row_ss, row_rs.at[step], mate).start()

    def stage_gate_up(chips, which, sem):
        gate = up = None
        for k in range(X):
            x = rows[k, chips].reshape(Y * CAP, 512)
            g = jnp.dot(x, wg[which, k * 512 : (k + 1) * 512, :], preferred_element_type=jnp.float32)
            v = jnp.dot(x, wu[which, k * 512 : (k + 1) * 512, :], preferred_element_type=jnp.float32)
            gate, up = (g, v) if k == 0 else (gate + g, up + v)
        h = gate / (1.0 + jnp.exp(-gate)) * up
        place = (tp, pair)[which]
        hid[place, chips] = h.reshape(Y, CAP, 256).astype(jnp.bfloat16)
        to_tp(hid.at[place, chips], hid.at[place, chips], hid_ss, sem, mate).start()

    def down(chips, weight):
        out = None
        for k in range(X):
            h = hid[k, chips].reshape(Y * CAP, 256)
            o = jnp.dot(h, weight(k), preferred_element_type=jnp.float32)
            out = o if k == 0 else out + o
        return out.astype(jnp.bfloat16)

    def stage_down(step):
        offset = pick_of(SEND, step)
        chips = source_chips(offset)
        res[chips] = down(chips, lambda k: wd[0, k * 256 : (k + 1) * 256, :]).reshape(Y, CAP, 512)

        @pl.loop(0, Y)
        def _(j):
            goal = lax.rem(z + Z - offset, Z) * Y + j

            @pl.when(goal * C != ep)
            def _():
                to_ep(res.at[goal], ret.at[ep], ret_ss.at[0], ret_rs.at[0, step], goal * C).start()

            @pl.when(goal * C == ep)
            def _():
                ret[ep] = res[goal]

    def stage_down_pair(step, part):
        offset = pick_of(BACK, step)
        chips = source_chips(offset)
        out = down(chips, lambda k: wd[1, k * 256 : (k + 1) * 256, SPANS[part]])
        res_pair[part][chips] = out.reshape(Y, CAP, -1)

        @pl.loop(0, Y)
        def _(j):
            goal = lax.rem(z + Z - offset, Z) * Y + j

            @pl.when(goal * C + 1 != ep)
            def _():
                src, dst = res_pair[part].at[goal], ret_pair[part].at[ep]
                to_ep(src, dst, ret_ss.at[1 + part], ret_rs.at[1 + part, step], goal * C + 1).start()

            @pl.when(goal * C + 1 == ep)
            def _():
                ret_pair[part][ep] = res_pair[part][goal]

    @pl.loop(0, Z)
    def _(plane):
        index = lax.broadcasted_iota(jnp.int32, (count, PLANE * CAP), 1) + plane * (PLANE * CAP)
        index = index.astype(jnp.float32)
        share = jnp.where(cols[0][:, 0:1] == index, cols[2][:, 0:1], 0.0)
        share = jnp.where(cols[1][:, 0:1] == index, cols[3][:, 0:1], share)
        high = share.astype(jnp.bfloat16)
        shares[0, plane] = high
        shares[1, plane] = (share - high.astype(jnp.float32)).astype(jnp.bfloat16)

    def weighted(plane, got):
        return jnp.dot(shares[0, plane], got, preferred_element_type=jnp.float32) + jnp.dot(
            shares[1, plane], got, preferred_element_type=jnp.float32
        )

    def stage_combine(step):
        offset = pick_of(SEND, step)
        plane = lax.rem(z + offset, Z)
        await_slabs(ret_rs.at[0, step], offset == 0)
        got = ret[pl.ds(plane * PLANE, PLANE)].reshape(PLANE * CAP, 512)
        acc[...] += weighted(plane, got)

    def stage_combine_pair(step, part):
        offset = pick_of(BACK, step)
        plane = lax.rem(z + offset, Z)

        @pl.when(offset == 0)
        def _():
            await_recv(ret_pair[part].at[pl.ds(0, PLANE - 1)], ret_rs.at[1 + part, step])

        @pl.when(offset != 0)
        def _():
            await_recv(ret_pair[part].at[pl.ds(0, PLANE)], ret_rs.at[1 + part, step])

        got = ret_pair[part][pl.ds(plane * PLANE, PLANE)].reshape(PLANE * CAP, -1)
        acc[:, SPANS[part]] += weighted(plane, got)

    acc[...] = jnp.zeros(acc.shape, jnp.float32)

    def stage_own(step):
        chips = source_chips(pick_of(SEND, step))
        await_recv(rows.at[pl.ds(2 * (1 - u), 2), chips], row_rs.at[step])
        stage_gate_up(chips, 0, hid_rs.at[0, step])

    def stage_pair(step):
        stage_gate_up(source_chips(pick_of(SEND, step)), 1, hid_rs.at[1, step])

    def stage_down_own(step):
        chips = source_chips(pick_of(SEND, step))
        await_recv(hid.at[mate, chips], hid_rs.at[0, step])
        await_recv(hid.at[far, chips], hid_rs.at[1, step])
        stage_down(step)

    @pl.loop(0, Z - 1)
    def _(s):
        stage_rows(s)

        @pl.when(s >= 1)
        def _():
            stage_own(s - 1)

    await_recv(wg.at[1], wt_rs.at[0])
    await_recv(wu.at[1], wt_rs.at[1])

    @pl.loop(0, EARLY)
    def _(s):
        stage_pair(s)

    stage_rows(Z - 1)
    stage_own(Z - 2)

    @pl.loop(EARLY, Z - 1)
    def _(s):
        stage_pair(s)

    @pl.loop(0, EARLY)
    def _(s):
        stage_down_own(s)

    stage_own(Z - 1)
    stage_pair(Z - 1)
    await_recv(mixer_block(pair), mix_rs.at[0])
    to_tp(mixer_block(pair), mixer_block(pair), mix_ss.at[2], mix_rs.at[2], mate).start()

    @pl.loop(EARLY, Z)
    def _(s):
        stage_down_own(s)

    await_recv(wd.at[1, :, half_a], wt_rs.at[2])

    @pl.loop(0, Z)
    def _(s):
        stage_down_pair(s, 0)

    def stage_mixer(block):
        m = mrows[block]
        at = pl.multiple_of(block * m.shape[0], 16)
        in_gate = jnp.dot(m, wi[...], preferred_element_type=jnp.float32)
        values = jnp.dot(m, wv[...], preferred_element_type=jnp.float32)
        ext[pl.ds(HALO + at, m.shape[0]), :] = (in_gate * values).astype(jnp.bfloat16).astype(jnp.float32)
        ogate[pl.ds(at, m.shape[0]), :] = jnp.dot(m, wo[...], preferred_element_type=jnp.float32)

    for load in loads[3:]:
        load.wait()
    await_recv(halo.at[1], halo_rs)
    in_gate = jnp.dot(halo[1], wi[...], preferred_element_type=jnp.float32)
    values = jnp.dot(halo[1], wv[...], preferred_element_type=jnp.float32)
    product = (in_gate * values).astype(jnp.bfloat16).astype(jnp.float32)
    ext[0:HALO, :] = jnp.where(ep == 0, 0.0, product)
    await_recv(mixer_block(mate), mix_rs.at[1])

    @pl.loop(0, X)
    def _(n):
        @pl.when(n == X - 1)
        def _():
            await_recv(mixer_block(far), mix_rs.at[2])

        stage_mixer(jnp.where(n == X - 1, far, jnp.where(n == 0, tp, jnp.where(n == 1, mate, pair))))

    for n in range(2):
        for i in range(2):
            lanes = slice(n * 256 + i * 128, n * 256 + (i + 1) * 128)
            tap_span = pl.ds(pl.multiple_of(tp * 512 + n * 256 + i * 128, 128), 128)
            conv = taps[0:1, tap_span] * ext[HALO - 2 : HALO - 2 + count, lanes]
            conv = conv + taps[1:2, tap_span] * ext[HALO - 1 : HALO - 1 + count, lanes]
            conv = conv + taps[2:3, tap_span] * ext[HALO:, lanes]
            gat[tp, n, :, i * 128 : (i + 1) * 128] = (ogate[:, lanes] * conv).astype(jnp.bfloat16)

        to_tp(gat.at[tp, n], gat.at[tp, n], gat_ss.at[0], gat_rs.at[0, n], pair).start()
        to_tp(gat.at[tp, n], gat.at[tp, n], gat_ss.at[1], gat_rs.at[1, n], mate).start()

    await_recv(wd.at[1, :, half_b], wt_rs.at[3])

    @pl.loop(0, Z)
    def _(s):
        stage_down_pair(s, 1)

    def gated_pass(n):
        await_recv(gat.at[pair, n], gat_rs.at[0, n])
        to_tp(gat.at[pair, n], gat.at[pair, n], gat_ss.at[2], gat_rs.at[2, n], mate).start()

    gated_pass(0)

    @pl.when(core == 0)
    def _():
        @pl.loop(0, Z)
        def _(s):
            stage_combine(s)

        fin[...] = acc[...].astype(jnp.bfloat16).reshape(C, count // 2, 512)
        to_ep(fin.at[1], fin_same, fin_ss.at[0], fin_rs.at[0], twin).start()

    def combine_pair(part, start, stop):
        @pl.when(core == 1)
        def _():
            @pl.loop(start, stop)
            def _(s):
                stage_combine_pair(s, part)

    def finish_pair(part):
        @pl.when(core == 1)
        def _():
            fin_half[part][...] = acc[:, SPANS[part]].astype(jnp.bfloat16).reshape(C, count // 2, -1)
            out, into = fin_half[part], fin_pair[part]
            to_twin(out.at[0], into, fin_ss.at[1 + part], fin_rs.at[1 + part], pair).start()
            to_tp(out.at[1], into, fin_ss.at[3 + part], fin_rs.at[1 + part], pair).start()

    combine_pair(0, 0, 4)
    gated_pass(1)
    combine_pair(0, 4, Z)
    finish_pair(0)
    combine_pair(1, 0, Z)
    finish_pair(1)
    for n in range(2):
        await_recv(gat.at[mate, n], gat_rs.at[1, n])
        await_recv(gat.at[far, n], gat_rs.at[2, n])

    @pl.loop(0, 2)
    def _(n):
        span = pl.ds(pl.multiple_of(n * 256, 256), 256)
        out = None
        for k in range(2 * X):
            part = gat[k // 2, k % 2]
            o = jnp.dot(part, wp[k * 256 : (k + 1) * 256, span], preferred_element_type=jnp.float32)
            out = o if k == 0 else out + o
        mixed[:, span] = out.astype(jnp.bfloat16)

    stores = [pltpu.make_async_copy(mixed, mixer_out, store_sem.at[0])]
    stores[0].start()

    own = count // 4

    def store_rows(src, block, span, at):
        for place in range(2):
            copy = pltpu.make_async_copy(
                src.at[pl.ds(place * own, own)],
                expert_out.at[lax.rem(first + block + place, X), :, span],
                store_sem.at[at + place],
            )
            copy.start()
            stores.append(copy)

    @pl.when(core == 1)
    def _():
        await_recv(fin_same, fin_rs.at[0])
        fin[0] = fin_same[...]

    store_rows(fin.at[0], 0, slice(None), 1)
    for part in range(2):
        await_recv(fin_pair[part], fin_rs.at[1 + part])
        store_rows(fin_pair[part], 2, SPANS[part], 3 + 2 * part)

    for copy in stores:
        copy.wait()

    @pl.when(core == 0)
    def _():
        await_send(fin.at[1], fin_ss.at[0])

    @pl.when(core == 1)
    def _():
        for part in range(2):
            await_send(fin_pair[part], fin_ss.at[1 + part])
            await_send(fin_pair[part], fin_ss.at[3 + part])

    await_send(route.at[0], route_ss)
    await_send(send.at[pl.ds(0, 12)], tok_ss)
    await_send(wg.at[0], wt_ss.at[0])
    await_send(wu.at[0], wt_ss.at[1])
    await_send(wd.at[0, :, half_a], wt_ss.at[2])
    await_send(wd.at[0, :, half_b], wt_ss.at[3])
    for i in range(3):
        await_send(mixer_block(0), mix_ss.at[i])
        await_send(gat.at[0], gat_ss.at[i])
    await_send(send.at[pl.ds(0, EP - 1)], disp_ss)
    await_send(rows.at[pl.ds(0, 2)], row_ss)
    await_send(hid.at[pl.ds(0, 2)], hid_ss)

    @pl.when(tp == X - 1)
    def _():
        for _ in range(X):
            await_send(halo.at[0], halo_ss)

    @pl.when(core == 0)
    def _():
        await_send(ret.at[pl.ds(0, CHIPS - 1)], ret_ss.at[0])
        await_send(ret_pair[0].at[pl.ds(0, CHIPS)], ret_ss.at[1])
        await_send(ret_pair[1].at[pl.ds(0, CHIPS)], ret_ss.at[2])

    @pl.when(core == 1)
    def _():
        await_send(ret.at[pl.ds(0, CHIPS)], ret_ss.at[0])
        await_send(ret_pair[0].at[pl.ds(0, CHIPS - 1)], ret_ss.at[1])
        await_send(ret_pair[1].at[pl.ds(0, CHIPS - 1)], ret_ss.at[2])


def hand_over(mixer_in, expert_in, mixer_out, expert_out, held, in_sem, out_sem):
    ins = [pltpu.make_async_copy(src, held.at[i], in_sem.at[i]) for i, src in enumerate((mixer_in, expert_in))]
    outs = [pltpu.make_async_copy(held.at[i], dst, out_sem.at[i]) for i, dst in enumerate((mixer_out, expert_out))]
    for copy in ins:
        copy.start()
    for i in range(2):
        ins[i].wait()
        outs[i].start()
    for copy in outs:
        copy.wait()


def on_device(
    mixer_in, expert_in, mixer_gain, in_gate_weight, out_gate_weight, value_weight, conv_taps, mixer_proj,
    expert_gain, route_ids, route_weights, gate_weight, up_weight, down_weight,
):
    bf16, f32 = jnp.bfloat16, jnp.float32
    own, wide = mixer_in.shape
    parts = [span.stop - span.start for span in SPANS]
    count = route_ids.shape[0]
    local = pl.BlockSpec(memory_space=pltpu.VMEM)
    remote = pl.BlockSpec(memory_space=pl.ANY)
    dma, vmem = pltpu.SemaphoreType.DMA, pltpu.VMEM
    out = jax.ShapeDtypeStruct((count, 512), bf16)
    results = pl.pallas_call(
        kernel,
        out_shape=(out, jax.ShapeDtypeStruct((X, own, 512), bf16)),
        in_specs=[local] * 7 + [remote] * 7,
        out_specs=(remote, remote),
        scratch_shapes=[
            *[vmem((wide, 512), bf16)] * 4, *[vmem((2, wide, 256), bf16)] * 2, vmem((2, 1024, 512), bf16),
            vmem((C, 8, count), f32), vmem((X, own, 512), bf16), vmem((C, 2, own, 512), bf16),
            vmem((X, own, wide), bf16), vmem((2, HALO, wide), bf16),
            vmem((EP, CAP, 512), bf16), vmem((X, CHIPS, CAP, 512), bf16), vmem((X, CHIPS, CAP, 256), bf16),
            vmem((CHIPS, CAP, 512), bf16), *[vmem((CHIPS, CAP, part), bf16) for part in parts],
            vmem((EP, CAP, 512), bf16), *[vmem((EP, CAP, part), bf16) for part in parts], vmem((X, 2, count, 256), bf16),
            vmem((HALO + count, 512), f32), vmem((count, 512), f32), vmem((count, 512), f32),
            vmem((8, count), f32), vmem((4, count, 128), f32),
            vmem((C, count // 2, 512), bf16), vmem((count // 2, 512), bf16),
            *[vmem((C, count // 2, part), bf16) for part in parts], *[vmem((count // 2, part), bf16) for part in parts],
            vmem((Z, PLANE * CAP, count), bf16), vmem((2, Z, count, PLANE * CAP), bf16), vmem((count, 512), bf16),
            dma((7,)), dma((7,)), dma((4,)), dma((4,)), dma, dma, dma, dma, dma((3,)), dma((3,)), dma, dma((Z,)), dma, dma((Z,)),
            dma, dma((2, Z)), dma((3,)), dma((3, Z)), dma((3,)), dma((3, 2)), dma, dma, dma((5,)), dma((3,)),
        ],
        compiler_params=pltpu.CompilerParams(
            collective_id=0, has_side_effects=True, vmem_limit_bytes=62 * 2**20
        ),
        name="mixer_and_experts",
    )(
        mixer_in, expert_in, mixer_gain.reshape(1, -1), expert_gain.reshape(1, -1), conv_taps,
        route_ids.T, route_weights.T,
        in_gate_weight, out_gate_weight, value_weight, mixer_proj, gate_weight[0], up_weight[0], down_weight[0],
    )
    return pl.pallas_call(
        hand_over,
        out_shape=(out, out),
        in_specs=[remote] * 2,
        out_specs=(remote, remote),
        scratch_shapes=[vmem((2, count, 512), bf16), dma((2,)), dma((2,))],
        name="hand_over",
    )(results[0], results[1].reshape(count, 512))


def solution(mesh):
    return jax.shard_map(
        on_device,
        mesh=mesh,
        in_specs=(
            P(("ep", "tp"), None),
            P(("ep", "tp"), None),
            P(),
            P(None, "tp"),
            P(None, "tp"),
            P(None, "tp"),
            P(),
            P(None, "tp"),
            P(),
            P("ep", None),
            P("ep", None),
            P("ep", None, "tp"),
            P("ep", None, "tp"),
            P("ep", None, "tp"),
        ),
        out_specs=(P("ep", "tp"), P("ep", "tp")),
        check_vma=False,
    )
```

```python
import jax
import jax.numpy as jnp
from jax import lax
from jax.experimental import pallas as pl
from jax.experimental.pallas import tpu as pltpu
from jax.sharding import PartitionSpec as P

norm_eps = 1e-06
Z, Y, C, X = 8, 4, 2, 4
PLANE = Y * C
EP = Z * PLANE
CHIPS = Z * Y
CAP = 24
SEND = (1, 7, 2, 6, 0, 3, 5, 4)
BACK = (4, 3, 5, 2, 6, 1, 7, 0)
SPANS = (slice(0, 256), slice(256, 512))
EARLY = 4
HALO = 8
MESH = pl.DeviceIdType.MESH


def pick_of(table, step):
    value = table[0]
    for at in range(1, len(table)):
        value = jnp.where(step == at, table[at], value)
    return value


def rms_rows(values, gain_row):
    wide = values.astype(jnp.float32)
    scale = lax.rsqrt(jnp.mean(wide * wide, axis=-1, keepdims=True) + norm_eps)
    return (wide * scale * gain_row).astype(jnp.bfloat16)


def kernel(
    mixer_in, expert_in, mixer_gain, expert_gain, taps, ids, weights,
    wi_hbm, wo_hbm, wv_hbm, wp_hbm, wg_hbm, wu_hbm, wd_hbm,
    mixer_out, expert_out,
    wi, wo, wv, wp, wg, wu, wd,
    route, tok_send, tok, mrows, halo, send, rows, hid, res, res_pair_a, res_pair_b, ret, ret_pair_a, ret_pair_b, gat, ext, ogate, acc, slot_rows, cols,
    fin, fin_same, fin_half_a, fin_half_b, fin_pair_a, fin_pair_b, picks_of, shares, mixed,
    load_sem, store_sem, wt_ss, wt_rs, route_ss, route_rs, tok_ss, tok_rs, mix_ss, mix_rs, disp_ss, disp_rs, row_ss, row_rs,
    hid_ss, hid_rs, ret_ss, ret_rs, gat_ss, gat_rs, halo_ss, halo_rs, fin_ss, fin_rs,
):
    ep, tp = lax.axis_index("ep"), lax.axis_index("tp")
    res_pair, ret_pair = (res_pair_a, res_pair_b), (ret_pair_a, ret_pair_b)
    fin_half, fin_pair = (fin_half_a, fin_half_b), (fin_pair_a, fin_pair_b)
    z, core = ep // PLANE, lax.rem(ep, C)
    chip, twin = ep // C, ep + 1 - 2 * core
    odd = lax.rem(tp, 2)
    pair = tp + 1 - 2 * odd
    mate = lax.rem(tp + 3 + 2 * odd, X)
    far = lax.rem(tp + 2, X)
    u = 1 - odd
    first = lax.rem(tp + X - u, X)
    count = ids.shape[1]

    loads = [
        pltpu.make_async_copy(src, dst, load_sem.at[i])
        for i, (src, dst) in enumerate(
            ((wg_hbm, wg.at[0]), (wu_hbm, wu.at[0]), (wd_hbm, wd.at[0]),
             (wi_hbm, wi), (wo_hbm, wo), (wv_hbm, wv), (wp_hbm, wp))
        )
    ]
    for load in loads:
        load.start()

    barrier = pltpu.get_barrier_semaphore()

    @pl.loop(1, EP)
    def _(d):
        pl.semaphore_signal(barrier, inc=1, device_id={"ep": lax.rem(ep + d, EP)}, device_id_type=MESH)

    for other in (pair, mate):
        pl.semaphore_signal(barrier, inc=1, device_id={"tp": other}, device_id_type=MESH)
        pl.semaphore_signal(barrier, inc=1, device_id={"ep": twin, "tp": other}, device_id_type=MESH)

    @pl.when(tp != X - 1)
    def _():
        pl.semaphore_signal(
            barrier, inc=1, device_id={"ep": lax.rem(ep + EP - 1, EP), "tp": X - 1}, device_id_type=MESH
        )

    def to_ep(src, dst, ss, rs, target):
        return pltpu.make_async_remote_copy(src, dst, ss, rs, device_id={"ep": target}, device_id_type=MESH)

    def to_tp(src, dst, ss, rs, target):
        return pltpu.make_async_remote_copy(src, dst, ss, rs, device_id={"tp": target}, device_id_type=MESH)

    def mixer_block(owner):
        return mrows.at[owner]

    def to_twin(src, dst, ss, rs, target):
        return pltpu.make_async_remote_copy(
            src, dst, ss, rs, device_id={"ep": twin, "tp": target}, device_id_type=MESH
        )

    def await_recv(ref, sem):
        to_tp(ref, ref, sem, sem, mate).wait_recv()

    def await_send(ref, sem):
        to_tp(ref, ref, sem, sem, mate).wait_send()

    picks = jnp.concatenate(
        [ids[...].astype(jnp.float32), weights[...], jnp.zeros((4, count), jnp.float32)], axis=0
    )
    turned = jnp.where((first == 1) == (core == 0), pltpu.roll(picks, 3 * count // 4, 1), pltpu.roll(picks, count // 4, 1))
    route[core] = turned
    normed = rms_rows(expert_in[...], expert_gain[...])
    for k in range(X):
        tok_send[k] = normed[:, k * 512 : (k + 1) * 512]
    tok[core, u] = tok_send[2 * u + core]

    for load in loads[:3]:
        load.wait()
    half_a, half_b = (pl.ds(span.start, span.stop - span.start) for span in SPANS)
    pl.semaphore_wait(barrier, EP + 3 + (X - 1) * (tp // (X - 1)))

    to_ep(route.at[core], route.at[core], route_ss, route_rs, twin).start()
    to_twin(tok_send.at[2 * (1 - u) + 1 - core], tok.at[core, u], tok_ss, tok_rs, mate).start()
    to_tp(tok_send.at[2 * (1 - u) + core], tok.at[core, u], tok_ss, tok_rs, mate).start()
    to_ep(tok_send.at[2 * u + 1 - core], tok.at[core, u], tok_ss, tok_rs, twin).start()
    tail_rows = rms_rows(mixer_in[mixer_in.shape[0] - 16 :], mixer_gain[...])
    halo[0] = tail_rows[16 - HALO :]

    @pl.when(tp == X - 1)
    def _():
        for other in range(X):
            pltpu.make_async_remote_copy(
                halo.at[0], halo.at[1], halo_ss, halo_rs,
                device_id={"ep": lax.rem(ep + 1, EP), "tp": other}, device_id_type=MESH,
            ).start()

    to_tp(wg.at[0], wg.at[1], wt_ss.at[0], wt_rs.at[0], pair).start()
    to_tp(wu.at[0], wu.at[1], wt_ss.at[1], wt_rs.at[1], pair).start()
    mrows[tp] = rms_rows(mixer_in[...], mixer_gain[...])
    to_tp(mixer_block(tp), mixer_block(tp), mix_ss.at[0], mix_rs.at[0], pair).start()
    to_tp(wd.at[0, :, half_a], wd.at[1, :, half_a], wt_ss.at[2], wt_rs.at[2], pair).start()
    to_tp(wd.at[0, :, half_b], wd.at[1, :, half_b], wt_ss.at[3], wt_rs.at[3], pair).start()

    await_recv(route.at[1 - core], route_rs)
    lane = lax.broadcasted_iota(jnp.int32, (8, count), 1)
    both = jnp.where(lane < count // 2, route[0], route[1])
    labels = lax.broadcasted_iota(jnp.int32, (EP, count), 0).astype(jnp.float32)
    hot = [both[k : k + 1, :] == labels for k in range(2)]
    named = jnp.where(hot[0] | hot[1], 1.0, 0.0).astype(jnp.bfloat16)
    older = (
        lax.broadcasted_iota(jnp.int32, (count, count), 0) < lax.broadcasted_iota(jnp.int32, (count, count), 1)
    )
    earlier = jnp.dot(named, jnp.where(older, 1.0, 0.0).astype(jnp.bfloat16), preferred_element_type=jnp.float32)
    for k in range(2):
        within = jnp.sum(jnp.where(hot[k], earlier, 0.0), axis=0, keepdims=True)
        slot = both[k : k + 1, :] * CAP + within
        slot_rows[k : k + 1, :] = slot

    @pl.loop(0, Z)
    def _(plane):
        index = (lax.broadcasted_iota(jnp.int32, (PLANE * CAP, count), 0) + plane * (PLANE * CAP)).astype(jnp.float32)
        pick = (index == slot_rows[0:1, :]) | (index == slot_rows[1:2, :])
        picks_of[plane] = jnp.where(pick, 1.0, 0.0).astype(jnp.bfloat16)

    await_recv(send.at[pl.ds(0, 12)], tok_rs)
    to_tp(mixer_block(tp), mixer_block(tp), mix_ss.at[1], mix_rs.at[1], mate).start()

    @pl.loop(0, Z)
    def _(step):
        plane = lax.rem(z + pick_of(SEND, step), Z)
        moved = jnp.dot(picks_of[plane], tok[...].reshape(count, 512), preferred_element_type=jnp.float32)
        send[pl.ds(plane * PLANE, PLANE)] = moved.reshape(PLANE, CAP, 512).astype(jnp.bfloat16)

        @pl.loop(0, PLANE)
        def _(j):
            target = plane * PLANE + j

            @pl.when(target != ep)
            def _():
                to_ep(send.at[target], rows.at[2 * u + core, chip], disp_ss, disp_rs.at[step], target).start()

            @pl.when(target == ep)
            def _():
                rows[2 * u + core, chip] = send[ep]

    total = both[2:3, :] + both[3:4, :]
    for k in range(2):
        cols[k] = jnp.transpose(jnp.broadcast_to(slot_rows[k : k + 1, :], (128, count)))
        cols[2 + k] = jnp.transpose(jnp.broadcast_to(both[2 + k : 3 + k, :] / total, (128, count)))

    def source_chips(offset):
        return pl.ds(lax.rem(z + Z - offset, Z) * Y, Y)

    def await_slabs(sem, last):
        @pl.when(last)
        def _():
            await_recv(send.at[pl.ds(0, PLANE - 1)], sem)

        @pl.when(jnp.logical_not(last))
        def _():
            await_recv(send.at[pl.ds(0, PLANE)], sem)

    def stage_rows(step):
        block = rows.at[pl.ds(2 * u, 2), source_chips(pick_of(SEND, step))]
        await_slabs(disp_rs.at[step], step == SEND.index(0))
        to_tp(block, block, row_ss, row_rs.at[step], mate).start()

    def stage_gate_up(chips, which, sem):
        gate = up = None
        for k in range(X):
            x = rows[k, chips].reshape(Y * CAP, 512)
            g = jnp.dot(x, wg[which, k * 512 : (k + 1) * 512, :], preferred_element_type=jnp.float32)
            v = jnp.dot(x, wu[which, k * 512 : (k + 1) * 512, :], preferred_element_type=jnp.float32)
            gate, up = (g, v) if k == 0 else (gate + g, up + v)
        h = gate / (1.0 + jnp.exp(-gate)) * up
        place = (tp, pair)[which]
        hid[place, chips] = h.reshape(Y, CAP, 256).astype(jnp.bfloat16)
        to_tp(hid.at[place, chips], hid.at[place, chips], hid_ss, sem, mate).start()

    def down(chips, weight):
        out = None
        for k in range(X):
            h = hid[k, chips].reshape(Y * CAP, 256)
            o = jnp.dot(h, weight(k), preferred_element_type=jnp.float32)
            out = o if k == 0 else out + o
        return out.astype(jnp.bfloat16)

    def stage_down(step):
        offset = pick_of(SEND, step)
        chips = source_chips(offset)
        res[chips] = down(chips, lambda k: wd[0, k * 256 : (k + 1) * 256, :]).reshape(Y, CAP, 512)

        @pl.loop(0, Y)
        def _(j):
            goal = lax.rem(z + Z - offset, Z) * Y + j

            @pl.when(goal * C != ep)
            def _():
                to_ep(res.at[goal], ret.at[ep], ret_ss.at[0], ret_rs.at[0, step], goal * C).start()

            @pl.when(goal * C == ep)
            def _():
                ret[ep] = res[goal]

    def stage_down_pair(step, part):
        offset = pick_of(BACK, step)
        chips = source_chips(offset)
        out = down(chips, lambda k: wd[1, k * 256 : (k + 1) * 256, SPANS[part]])
        res_pair[part][chips] = out.reshape(Y, CAP, -1)

        @pl.loop(0, Y)
        def _(j):
            goal = lax.rem(z + Z - offset, Z) * Y + j

            @pl.when(goal * C + 1 != ep)
            def _():
                src, dst = res_pair[part].at[goal], ret_pair[part].at[ep]
                to_ep(src, dst, ret_ss.at[1 + part], ret_rs.at[1 + part, step], goal * C + 1).start()

            @pl.when(goal * C + 1 == ep)
            def _():
                ret_pair[part][ep] = res_pair[part][goal]

    @pl.loop(0, Z)
    def _(plane):
        index = lax.broadcasted_iota(jnp.int32, (count, PLANE * CAP), 1) + plane * (PLANE * CAP)
        index = index.astype(jnp.float32)
        share = jnp.where(cols[0][:, 0:1] == index, cols[2][:, 0:1], 0.0)
        share = jnp.where(cols[1][:, 0:1] == index, cols[3][:, 0:1], share)
        high = share.astype(jnp.bfloat16)
        shares[0, plane] = high
        shares[1, plane] = (share - high.astype(jnp.float32)).astype(jnp.bfloat16)

    def weighted(plane, got):
        return jnp.dot(shares[0, plane], got, preferred_element_type=jnp.float32) + jnp.dot(
            shares[1, plane], got, preferred_element_type=jnp.float32
        )

    def stage_combine(step):
        offset = pick_of(SEND, step)
        plane = lax.rem(z + offset, Z)
        await_slabs(ret_rs.at[0, step], offset == 0)
        got = ret[pl.ds(plane * PLANE, PLANE)].reshape(PLANE * CAP, 512)
        acc[...] += weighted(plane, got)

    def stage_combine_pair(step, part):
        offset = pick_of(BACK, step)
        plane = lax.rem(z + offset, Z)

        @pl.when(offset == 0)
        def _():
            await_recv(ret_pair[part].at[pl.ds(0, PLANE - 1)], ret_rs.at[1 + part, step])

        @pl.when(offset != 0)
        def _():
            await_recv(ret_pair[part].at[pl.ds(0, PLANE)], ret_rs.at[1 + part, step])

        got = ret_pair[part][pl.ds(plane * PLANE, PLANE)].reshape(PLANE * CAP, -1)
        acc[:, SPANS[part]] += weighted(plane, got)

    acc[...] = jnp.zeros(acc.shape, jnp.float32)

    def stage_own(step):
        chips = source_chips(pick_of(SEND, step))
        await_recv(rows.at[pl.ds(2 * (1 - u), 2), chips], row_rs.at[step])
        stage_gate_up(chips, 0, hid_rs.at[0, step])

    def stage_pair(step):
        stage_gate_up(source_chips(pick_of(SEND, step)), 1, hid_rs.at[1, step])

    def stage_down_own(step):
        chips = source_chips(pick_of(SEND, step))
        await_recv(hid.at[mate, chips], hid_rs.at[0, step])
        await_recv(hid.at[far, chips], hid_rs.at[1, step])
        stage_down(step)

    @pl.loop(0, Z - 1)
    def _(s):
        stage_rows(s)

        @pl.when(s >= 1)
        def _():
            stage_own(s - 1)

    await_recv(wg.at[1], wt_rs.at[0])
    await_recv(wu.at[1], wt_rs.at[1])

    @pl.loop(0, EARLY)
    def _(s):
        stage_pair(s)

    stage_rows(Z - 1)
    stage_own(Z - 2)

    @pl.loop(EARLY, Z - 1)
    def _(s):
        stage_pair(s)

    @pl.loop(0, EARLY)
    def _(s):
        stage_down_own(s)

    stage_own(Z - 1)
    stage_pair(Z - 1)
    await_recv(mixer_block(pair), mix_rs.at[0])
    to_tp(mixer_block(pair), mixer_block(pair), mix_ss.at[2], mix_rs.at[2], mate).start()

    @pl.loop(EARLY, Z)
    def _(s):
        stage_down_own(s)

    await_recv(wd.at[1, :, half_a], wt_rs.at[2])

    @pl.loop(0, Z)
    def _(s):
        stage_down_pair(s, 0)

    def stage_mixer(block):
        m = mrows[block]
        at = pl.multiple_of(block * m.shape[0], 16)
        in_gate = jnp.dot(m, wi[...], preferred_element_type=jnp.float32)
        values = jnp.dot(m, wv[...], preferred_element_type=jnp.float32)
        ext[pl.ds(HALO + at, m.shape[0]), :] = (in_gate * values).astype(jnp.bfloat16).astype(jnp.float32)
        ogate[pl.ds(at, m.shape[0]), :] = jnp.dot(m, wo[...], preferred_element_type=jnp.float32)

    for load in loads[3:]:
        load.wait()
    await_recv(halo.at[1], halo_rs)
    in_gate = jnp.dot(halo[1], wi[...], preferred_element_type=jnp.float32)
    values = jnp.dot(halo[1], wv[...], preferred_element_type=jnp.float32)
    product = (in_gate * values).astype(jnp.bfloat16).astype(jnp.float32)
    ext[0:HALO, :] = jnp.where(ep == 0, 0.0, product)
    await_recv(mixer_block(mate), mix_rs.at[1])

    @pl.loop(0, X)
    def _(n):
        @pl.when(n == X - 1)
        def _():
            await_recv(mixer_block(far), mix_rs.at[2])

        stage_mixer(jnp.where(n == X - 1, far, jnp.where(n == 0, tp, jnp.where(n == 1, mate, pair))))

    for n in range(2):
        for i in range(2):
            lanes = slice(n * 256 + i * 128, n * 256 + (i + 1) * 128)
            tap_span = pl.ds(pl.multiple_of(tp * 512 + n * 256 + i * 128, 128), 128)
            conv = taps[0:1, tap_span] * ext[HALO - 2 : HALO - 2 + count, lanes]
            conv = conv + taps[1:2, tap_span] * ext[HALO - 1 : HALO - 1 + count, lanes]
            conv = conv + taps[2:3, tap_span] * ext[HALO:, lanes]
            gat[tp, n, :, i * 128 : (i + 1) * 128] = (ogate[:, lanes] * conv).astype(jnp.bfloat16)

        to_tp(gat.at[tp, n], gat.at[tp, n], gat_ss.at[0], gat_rs.at[0, n], pair).start()
        to_tp(gat.at[tp, n], gat.at[tp, n], gat_ss.at[1], gat_rs.at[1, n], mate).start()

    await_recv(wd.at[1, :, half_b], wt_rs.at[3])

    @pl.loop(0, Z)
    def _(s):
        stage_down_pair(s, 1)

    def gated_pass(n):
        await_recv(gat.at[pair, n], gat_rs.at[0, n])
        to_tp(gat.at[pair, n], gat.at[pair, n], gat_ss.at[2], gat_rs.at[2, n], mate).start()

    gated_pass(0)

    @pl.when(core == 0)
    def _():
        @pl.loop(0, Z)
        def _(s):
            stage_combine(s)

        fin[...] = acc[...].astype(jnp.bfloat16).reshape(C, count // 2, 512)
        to_ep(fin.at[1], fin_same, fin_ss.at[0], fin_rs.at[0], twin).start()

    def combine_pair(part, start, stop):
        @pl.when(core == 1)
        def _():
            @pl.loop(start, stop)
            def _(s):
                stage_combine_pair(jnp.where(s == 0, 0, jnp.where(s == Z - 1, 1, s + 1)), part)

    def finish_pair(part):
        @pl.when(core == 1)
        def _():
            fin_half[part][...] = acc[:, SPANS[part]].astype(jnp.bfloat16).reshape(C, count // 2, -1)
            out, into = fin_half[part], fin_pair[part]
            to_twin(out.at[0], into, fin_ss.at[1 + part], fin_rs.at[1 + part], pair).start()
            to_tp(out.at[1], into, fin_ss.at[3 + part], fin_rs.at[1 + part], pair).start()

    combine_pair(0, 0, 4)
    gated_pass(1)
    combine_pair(0, 4, Z)
    finish_pair(0)
    combine_pair(1, 0, Z)
    finish_pair(1)
    for n in range(2):
        await_recv(gat.at[mate, n], gat_rs.at[1, n])
        await_recv(gat.at[far, n], gat_rs.at[2, n])

    @pl.loop(0, 2)
    def _(n):
        span = pl.ds(pl.multiple_of(n * 256, 256), 256)
        out = None
        for k in range(2 * X):
            part = gat[k // 2, k % 2]
            o = jnp.dot(part, wp[k * 256 : (k + 1) * 256, span], preferred_element_type=jnp.float32)
            out = o if k == 0 else out + o
        mixed[:, span] = out.astype(jnp.bfloat16)

    stores = [pltpu.make_async_copy(mixed, mixer_out, store_sem.at[0])]
    stores[0].start()

    own = count // 4

    def store_rows(src, block, span, at):
        for place in range(2):
            copy = pltpu.make_async_copy(
                src.at[pl.ds(place * own, own)],
                expert_out.at[lax.rem(first + block + place, X), :, span],
                store_sem.at[at + place],
            )
            copy.start()
            stores.append(copy)

    @pl.when(core == 1)
    def _():
        await_recv(fin_same, fin_rs.at[0])
        fin[0] = fin_same[...]

    store_rows(fin.at[0], 0, slice(None), 1)
    for part in range(2):
        await_recv(fin_pair[part], fin_rs.at[1 + part])
        store_rows(fin_pair[part], 2, SPANS[part], 3 + 2 * part)

    for copy in stores:
        copy.wait()

    @pl.when(core == 0)
    def _():
        await_send(fin.at[1], fin_ss.at[0])

    @pl.when(core == 1)
    def _():
        for part in range(2):
            await_send(fin_pair[part], fin_ss.at[1 + part])
            await_send(fin_pair[part], fin_ss.at[3 + part])

    await_send(route.at[0], route_ss)
    await_send(send.at[pl.ds(0, 12)], tok_ss)
    await_send(wg.at[0], wt_ss.at[0])
    await_send(wu.at[0], wt_ss.at[1])
    await_send(wd.at[0, :, half_a], wt_ss.at[2])
    await_send(wd.at[0, :, half_b], wt_ss.at[3])
    for i in range(3):
        await_send(mixer_block(0), mix_ss.at[i])
        await_send(gat.at[0], gat_ss.at[i])
    await_send(send.at[pl.ds(0, EP - 1)], disp_ss)
    await_send(rows.at[pl.ds(0, 2)], row_ss)
    await_send(hid.at[pl.ds(0, 2)], hid_ss)

    @pl.when(tp == X - 1)
    def _():
        for _ in range(X):
            await_send(halo.at[0], halo_ss)

    @pl.when(core == 0)
    def _():
        await_send(ret.at[pl.ds(0, CHIPS - 1)], ret_ss.at[0])
        await_send(ret_pair[0].at[pl.ds(0, CHIPS)], ret_ss.at[1])
        await_send(ret_pair[1].at[pl.ds(0, CHIPS)], ret_ss.at[2])

    @pl.when(core == 1)
    def _():
        await_send(ret.at[pl.ds(0, CHIPS)], ret_ss.at[0])
        await_send(ret_pair[0].at[pl.ds(0, CHIPS - 1)], ret_ss.at[1])
        await_send(ret_pair[1].at[pl.ds(0, CHIPS - 1)], ret_ss.at[2])


def hand_over(mixer_in, expert_in, mixer_out, expert_out, held, in_sem, out_sem):
    ins = [pltpu.make_async_copy(src, held.at[i], in_sem.at[i]) for i, src in enumerate((mixer_in, expert_in))]
    outs = [pltpu.make_async_copy(held.at[i], dst, out_sem.at[i]) for i, dst in enumerate((mixer_out, expert_out))]
    for copy in ins:
        copy.start()
    for i in range(2):
        ins[i].wait()
        outs[i].start()
    for copy in outs:
        copy.wait()


def on_device(
    mixer_in, expert_in, mixer_gain, in_gate_weight, out_gate_weight, value_weight, conv_taps, mixer_proj,
    expert_gain, route_ids, route_weights, gate_weight, up_weight, down_weight,
):
    bf16, f32 = jnp.bfloat16, jnp.float32
    own, wide = mixer_in.shape
    parts = [span.stop - span.start for span in SPANS]
    count = route_ids.shape[0]
    local = pl.BlockSpec(memory_space=pltpu.VMEM)
    remote = pl.BlockSpec(memory_space=pl.ANY)
    dma, vmem = pltpu.SemaphoreType.DMA, pltpu.VMEM
    out = jax.ShapeDtypeStruct((count, 512), bf16)
    results = pl.pallas_call(
        kernel,
        out_shape=(out, jax.ShapeDtypeStruct((X, own, 512), bf16)),
        in_specs=[local] * 7 + [remote] * 7,
        out_specs=(remote, remote),
        scratch_shapes=[
            *[vmem((wide, 512), bf16)] * 4, *[vmem((2, wide, 256), bf16)] * 2, vmem((2, 1024, 512), bf16),
            vmem((C, 8, count), f32), vmem((X, own, 512), bf16), vmem((C, 2, own, 512), bf16),
            vmem((X, own, wide), bf16), vmem((2, HALO, wide), bf16),
            vmem((EP, CAP, 512), bf16), vmem((X, CHIPS, CAP, 512), bf16), vmem((X, CHIPS, CAP, 256), bf16),
            vmem((CHIPS, CAP, 512), bf16), *[vmem((CHIPS, CAP, part), bf16) for part in parts],
            vmem((EP, CAP, 512), bf16), *[vmem((EP, CAP, part), bf16) for part in parts], vmem((X, 2, count, 256), bf16),
            vmem((HALO + count, 512), f32), vmem((count, 512), f32), vmem((count, 512), f32),
            vmem((8, count), f32), vmem((4, count, 128), f32),
            vmem((C, count // 2, 512), bf16), vmem((count // 2, 512), bf16),
            *[vmem((C, count // 2, part), bf16) for part in parts], *[vmem((count // 2, part), bf16) for part in parts],
            vmem((Z, PLANE * CAP, count), bf16), vmem((2, Z, count, PLANE * CAP), bf16), vmem((count, 512), bf16),
            dma((7,)), dma((7,)), dma((4,)), dma((4,)), dma, dma, dma, dma, dma((3,)), dma((3,)), dma, dma((Z,)), dma, dma((Z,)),
            dma, dma((2, Z)), dma((3,)), dma((3, Z)), dma((3,)), dma((3, 2)), dma, dma, dma((5,)), dma((3,)),
        ],
        compiler_params=pltpu.CompilerParams(
            collective_id=0, has_side_effects=True, vmem_limit_bytes=62 * 2**20
        ),
        name="mixer_and_experts",
    )(
        mixer_in, expert_in, mixer_gain.reshape(1, -1), expert_gain.reshape(1, -1), conv_taps,
        route_ids.T, route_weights.T,
        in_gate_weight, out_gate_weight, value_weight, mixer_proj, gate_weight[0], up_weight[0], down_weight[0],
    )
    return pl.pallas_call(
        hand_over,
        out_shape=(out, out),
        in_specs=[remote] * 2,
        out_specs=(remote, remote),
        scratch_shapes=[vmem((2, count, 512), bf16), dma((2,)), dma((2,))],
        name="hand_over",
    )(results[0], results[1].reshape(count, 512))


def solution(mesh):
    return jax.shard_map(
        on_device,
        mesh=mesh,
        in_specs=(
            P(("ep", "tp"), None),
            P(("ep", "tp"), None),
            P(),
            P(None, "tp"),
            P(None, "tp"),
            P(None, "tp"),
            P(),
            P(None, "tp"),
            P(),
            P("ep", None),
            P("ep", None),
            P("ep", None, "tp"),
            P("ep", None, "tp"),
            P("ep", None, "tp"),
        ),
        out_specs=(P("ep", "tp"), P("ep", "tp")),
        check_vma=False,
    )
```
